32 devices in a mesh: rep: 2 (over y), fs: 4 (over z), tp: 4 (over x, core).
Axes of the slice: x: 2, y: 2, z: 4, core: 2. Of those that a mesh axis runs over, the one named last changes fastest.
Arguments:
- stream: bfloat16 [4096, 2048], P(('rep', 'fs', 'tp')), may hold values from -6 to 6
- gain_before: float32 [2048], replicated, may hold values from 0.1 to 1.9
- gain_after: float32 [2048], replicated, may hold values from 0.1 to 1.9
- proj_gate: bfloat16 [2048, 3584], P('fs', 'tp'), may hold values from -0.125 to 0.125
- proj_lift: bfloat16 [2048, 3584], P('fs', 'tp'), may hold values from -0.125 to 0.125
- proj_down: bfloat16 [3584, 2048], P('tp', 'fs'), may hold values from -0.09375 to 0.09375
- mixer_gain: float32 [2048], replicated, may hold values from 0.1 to 1.9
- mixer_u: bfloat16 [2048, 2048], P('fs', 'tp'), may hold values from -0.125 to 0.125
- mixer_v: bfloat16 [2048, 2048], P('fs', 'tp'), may hold values from -1 to 1
- layer_gain: float32 [2048], P('tp'), may hold values from 0.1 to 1.9
- layer_shift: float32 [2048], P('tp'), may hold values from -3 to 3
- spatial: bfloat16 [16, 128, 128], P('tp'), may hold values from -0.5 to 0.5
- spatial_shift: float32 [16, 128], P('tp'), may hold values from 0.2 to 2
- mixer_down: bfloat16 [2048, 2048], P('tp', 'fs'), may hold values from -0.125 to 0.125
Outputs:
- result: bfloat16 [4096, 2048], P(('rep', 'fs', 'tp'))
The draws below stay inside these ranges and needn't reach their ends.
All inputs are finite; a program needn't handle non-finite values.
Results may differ from the reference program's by a relative error of at most 0.017.
Values may be sent and summed in bfloat16 or wider, within the bound.
A program may use at most 128 MiB of HBM per device.

```python
import jax
import jax.numpy as jnp
from jax import lax

D = 2048
FF = 3584
GROUPS = 16
GROUP_DIM = 128
SPAN = 128
TOK = 512
A = 2048
TOKENS = 4096
N_TP = 4


def draw_mixer_v(key, part):
    first_key, second_key = jax.random.split(key)
    position = jnp.arange(A, dtype=jnp.float32) / (A - 1)
    rising = 4.0
    basis = jnp.clip(jax.random.normal(first_key, (D, A), jnp.float32), -4.0, 4.0)
    jitter = jnp.exp(jax.random.uniform(second_key, (A,), jnp.float32, -0.3, 0.3))
    column_scale = rising ** (position - 0.5) * jitter
    return jnp.clip(basis * column_scale * D ** (-0.5), -1.0, 1.0).astype(jnp.bfloat16)


def levels(own_key, dims, pieces, low, high):
    def one(dim, blocks):
        draws = jax.random.uniform(jax.random.fold_in(jax.random.fold_in(own_key, 6), dim), (blocks,), jnp.float32, low / len(pieces), high / len(pieces))
        return jnp.repeat(jnp.exp(draws), dims[dim] // blocks).reshape((-1,) + (1,) * (len(dims) - dim - 1))

    factor_of = one(*pieces[0])
    for cut in pieces[1:]:
        factor_of = factor_of * one(*cut)
    return factor_of


def noise(rng, extent, scale, reach, shards=(), kind=jnp.bfloat16):
    result = scale * jax.random.normal(rng, extent, jnp.float32)
    if shards:
        result = result * levels(rng, extent, shards, -0.22, 0.18)
    return jnp.clip(result, -reach, reach).astype(kind)


def setup_inputs(seed: int = 0) -> dict:
    keys = jax.random.split(jax.random.key(seed), 15)
    stream = noise(keys[0], (TOKENS, D), 1.0, 6.0, ((0, 32),))
    gain_before = jnp.clip(1.0 + 0.18 * jax.random.normal(keys[1], (D,), jnp.float32), 0.1, 1.9)
    gain_after = jnp.clip(1.0 + 0.18 * jax.random.normal(keys[2], (D,), jnp.float32), 0.1, 1.9)
    proj_gate = noise(keys[3], (D, FF), D ** -0.5, 0.125, ((0, 4), (1, 4)))
    proj_lift = noise(keys[4], (D, FF), D ** -0.5, 0.125, ((0, 4), (1, 4)))
    proj_down = noise(keys[5], (FF, D), FF ** -0.5, 0.09375, ((0, 4), (1, 4)))
    mixer_gain = jnp.clip(1.0 + 0.18 * jax.random.normal(keys[6], (D,), jnp.float32), 0.1, 1.9)
    mixer_u = noise(keys[7], (D, A), D ** -0.5, 0.125, ((0, 4), (1, 4)))
    mixer_v = draw_mixer_v(jax.random.fold_in(keys[14], 71), 0)
    layer_gain = jnp.clip(1.0 + 0.18 * jax.random.normal(keys[9], (A,), jnp.float32), 0.1, 1.9)
    layer_shift = noise(keys[10], (A,), 0.5, 3.0, ((0, 4),), jnp.float32)
    spatial = noise(keys[11], (GROUPS, SPAN, SPAN), SPAN ** -0.5, 0.5, ((0, 4),))
    spatial_shift = jnp.clip(0.2 + 1.8 * jax.random.uniform(keys[12], (GROUPS, SPAN), jnp.float32) ** levels(keys[12], (GROUPS, SPAN), ((0, 4),), -0.2, 0.2), 0.2, 2.0)
    mixer_down = noise(keys[13], (A, D), A ** -0.5, 0.125, ((0, 4), (1, 4)))
    return {"stream": stream, "gain_before": gain_before, "gain_after": gain_after, "proj_gate": proj_gate, "proj_lift": proj_lift, "proj_down": proj_down, "mixer_gain": mixer_gain, "mixer_u": mixer_u, "mixer_v": mixer_v, "layer_gain": layer_gain, "layer_shift": layer_shift, "spatial": spatial, "spatial_shift": spatial_shift, "mixer_down": mixer_down}


norm_epsilon = 1e-06
layer_epsilon = 1e-05

def norm_rows(row_block, scale_gain):
    widened = row_block.astype(jnp.float32)
    factor = lax.rsqrt(lax.optimization_barrier(jnp.mean(widened * widened, axis=1, keepdims=True)) + norm_epsilon)
    return (widened * factor * scale_gain).astype(jnp.bfloat16)

def blocked_sum(left_rows, right_rows):
    unit_count = left_rows.shape[1] // N_TP
    running = jnp.zeros((left_rows.shape[0], right_rows.shape[1]), jnp.float32)
    for member in range(N_TP):
        partial_value = jnp.dot(left_rows[:, member * unit_count:(member + 1) * unit_count], right_rows[member * unit_count:(member + 1) * unit_count], preferred_element_type=jnp.float32)
        running = running + lax.optimization_barrier(partial_value.astype(jnp.bfloat16)).astype(jnp.float32)
    return running

def half_step(row_block, scale_gain, proj_gate, proj_lift, proj_down):
    normed = norm_rows(row_block, scale_gain)
    gate_vals = jnp.dot(normed, proj_gate, preferred_element_type=jnp.float32)
    lift_vals = jnp.dot(normed, proj_lift, preferred_element_type=jnp.float32)
    hidden = (jax.nn.silu(gate_vals) * lift_vals).astype(jnp.bfloat16)
    delta = blocked_sum(hidden, proj_down)
    return (row_block.astype(jnp.float32) + 0.5 * delta).astype(jnp.bfloat16)

def token_mixer(row_block, mixer_gain, mixer_u, mixer_v, layer_gain, layer_shift, spatial, spatial_shift, mixer_down):
    normed = norm_rows(row_block, mixer_gain)
    u_vals = jnp.dot(normed, mixer_u, preferred_element_type=jnp.float32)
    v_vals = jnp.dot(normed, mixer_v, preferred_element_type=jnp.float32)
    lifted = jax.nn.gelu(v_vals)
    centre = lax.optimization_barrier(jnp.mean(lifted, axis=1, keepdims=True))
    spread = lax.optimization_barrier(jnp.mean(jnp.square(lifted - centre), axis=1, keepdims=True))
    normed_v = ((lifted - centre) * lax.rsqrt(spread + layer_epsilon) * layer_gain + layer_shift).astype(jnp.bfloat16)
    blocked = normed_v.reshape(TOK // SPAN, SPAN, GROUPS, GROUP_DIM).astype(jnp.float32)
    causal = jnp.tril(jnp.ones((SPAN, SPAN), dtype=bool))
    masked = jnp.where(causal[None], spatial.astype(jnp.float32), jnp.float32(0.0))
    mixed_v = jnp.einsum('gts,bsgd->btgd', masked, blocked) + spatial_shift.T[None, :, :, None]
    gated = (jax.nn.gelu(u_vals) * mixed_v.reshape(TOK, GROUPS * GROUP_DIM)).astype(jnp.bfloat16)
    delta = blocked_sum(gated, mixer_down)
    return (row_block.astype(jnp.float32) + delta).astype(jnp.bfloat16)

def reference(stream, gain_before, gain_after, proj_gate, proj_lift, proj_down, mixer_gain, mixer_u, mixer_v, layer_gain, layer_shift, spatial, spatial_shift, mixer_down):

    def one_sequence(row_block):
        first = half_step(row_block, gain_before, proj_gate, proj_lift, proj_down)
        second = token_mixer(first, mixer_gain, mixer_u, mixer_v, layer_gain, layer_shift, spatial, spatial_shift, mixer_down)
        return half_step(second, gain_after, proj_gate, proj_lift, proj_down)
    stacked = stream.reshape(stream.shape[0] // TOK, TOK, stream.shape[1])
    return lax.map(one_sequence, stacked).reshape(stream.shape)
```

```python
import functools

import jax
import jax.numpy as jnp
from jax import lax
from jax.experimental import pallas as pl
from jax.experimental.pallas import tpu as pltpu
from jax.sharding import PartitionSpec as P

SPAN = 128

norm_epsilon = 1e-06
layer_epsilon = 1e-05

MESH = pl.DeviceIdType.MESH
GATE, LIFT, DOWN, MIX_U, MIX_V, MIX_DOWN = range(6)
CUTS = 2
AHEAD = 3
NEAR = 1
HALVES = 2
MIXERS = (MIX_U, MIX_V, MIX_DOWN)
BY_ROWS = (GATE, LIFT, MIX_U, MIX_V)


def norm_rows(widened, scale_gain):
    factor = lax.rsqrt(jnp.mean(widened * widened, axis=1, keepdims=True) + norm_epsilon)
    return (widened * factor * scale_gain).astype(jnp.bfloat16)


def layer_kernel(
    n_rep,
    n_fs,
    n_tp,
    stream,
    gain_before,
    gain_after,
    mixer_gain,
    layer_gain,
    layer_shift,
    spatial,
    spatial_shift,
    proj_gate,
    proj_lift,
    proj_down,
    mixer_u,
    mixer_v,
    mixer_down,
    out,
    gate_all,
    lift_all,
    down_all,
    u_all,
    v_all,
    mix_down_all,
    rows_all,
    to_sibling,
    from_sibling,
    to_chip,
    from_chip,
    part,
    hold,
    gate_vals,
    hidden,
    u_vals,
    lifted,
    gated,
    rows_last,
    hidden_last,
    part_half,
    masked,
    mom_own,
    mom_in,
    square,
    resid,
    local_sem,
    z_send,
    z_recv,
    y_send,
    y_recv,
    ag_sem,
    agf_sem,
    sib_sem,
    chip_sem,
    mom_sem,
    token_sem,
    second_sem,
    agl_sem,
    last_sem,
):
    rep, fs, tp = lax.axis_index("rep"), lax.axis_index("fs"), lax.axis_index("tp")
    chip, core = tp // 2, lax.rem(tp, 2)
    n_chip = n_tp // 2
    block, width = stream.shape
    pair = 2 * block
    cols = width // n_fs
    shards = (proj_gate, proj_lift, proj_down, mixer_u, mixer_v, mixer_down)
    full = (gate_all, lift_all, down_all, u_all, v_all, mix_down_all)
    mine = pl.ds(pl.multiple_of(core * block, block), block)
    theirs = pl.ds(pl.multiple_of((1 - core) * block, block), block)
    sibling = chip * 2 + (1 - core)

    spread = n_fs >= 4
    depth = jnp.minimum(fs, n_fs - 1 - fs)
    side = (2 * fs) // n_fs
    inward = 1 - 2 * side
    if spread:
        low_slot = lax.rem(jnp.minimum(depth, 2) + 2, 3)
        at_end, at_mid = depth == 0, depth == 1
    else:
        low_slot = 1
    busy = low_slot < 2

    def when_busy(run):
        if spread:
            pl.when(busy)(run)
        else:
            run()

    def when_mid(run):
        if spread:
            pl.when(at_mid)(run)

    def when_end(run):
        if spread:
            pl.when(at_end)(run)

    def low_depth(w):
        return 1 if spread and w in MIXERS else 0

    def at(r, f, t):
        return (r, f, t)

    barrier = pltpu.get_barrier_semaphore()

    @pl.when(fs > 0)
    def _():
        pl.semaphore_signal(barrier, inc=1, device_id=at(rep, fs - 1, tp), device_id_type=MESH)

    @pl.when(fs < n_fs - 1)
    def _():
        pl.semaphore_signal(barrier, inc=1, device_id=at(rep, fs + 1, tp), device_id_type=MESH)

    for k in range(1, n_rep):
        pl.semaphore_signal(
            barrier, inc=1, device_id=at(lax.rem(rep + k, n_rep), fs, tp), device_id_type=MESH
        )
    for k in range(1, n_tp):
        pl.semaphore_signal(
            barrier, inc=1, device_id=at(rep, fs, lax.rem(tp + k, n_tp)), device_id_type=MESH
        )

    def depth_of(w):
        return shards[w].shape[0]

    def whole(w, owner):
        if w in BY_ROWS:
            n = depth_of(w)
            return full[w].at[pl.ds(pl.multiple_of(owner * n, n), n)]
        return full[w].at[owner]

    locals_ = [
        pltpu.make_async_copy(shards[w], whole(w, fs), local_sem.at[w]) for w in range(6)
    ]
    for copy in locals_:
        copy.start()

    line_peers = jnp.minimum(fs, 1) + jnp.minimum(n_fs - 1 - fs, 1)
    pl.semaphore_wait(barrier, n_rep - 1 + n_tp - 1 + line_peers)

    items = 6 * CUTS

    def piece(i, owner, part_index):
        w, cut = i // CUTS, i % CUTS
        rows = depth_of(w) // (n_rep * CUTS)
        first_row = (part_index * CUTS + cut) * rows
        if w in BY_ROWS:
            start = pl.multiple_of(owner * depth_of(w) + first_row, rows)
            return full[w].at[pl.ds(start, rows)]
        return full[w].at[owner, pl.ds(pl.multiple_of(first_row, rows), rows)]

    def z_copy(i, owner, out):
        ref = piece(i, owner, rep)
        step = inward if out == 0 else -inward
        return pltpu.make_async_remote_copy(
            src_ref=ref, dst_ref=ref, send_sem=z_send.at[out, i, owner],
            recv_sem=z_recv.at[i, owner],
            device_id=at(rep, fs + step, tp), device_id_type=MESH,
        )

    def rest_copy(i, k):
        ref = piece(i, fs, lax.rem(rep + n_rep - k, n_rep))
        return pltpu.make_async_remote_copy(
            src_ref=ref, dst_ref=ref, send_sem=y_send.at[i, k - 1, fs],
            recv_sem=y_recv.at[i, k - 1, fs],
            device_id=at(rep, fs + inward, tp), device_id_type=MESH,
        )

    def y_copy(i, owner, k):
        ref = piece(i, owner, rep)
        return pltpu.make_async_remote_copy(
            src_ref=ref, dst_ref=ref, send_sem=y_send.at[i, k - 1, owner],
            recv_sem=y_recv.at[i, k - 1, owner],
            device_id=at(lax.rem(rep + k, n_rep), fs, tp), device_id_type=MESH,
        )

    def own(i):
        w = i // CUTS
        if i % CUTS == 0:
            locals_[w].wait()
        if n_fs > 1:
            z_copy(i, fs, 0).start()

        @pl.when(depth > low_depth(w))
        def _():
            z_copy(i, fs, 1).start()

    def own_end(i):
        own(i)
        for k in range(1, n_rep):
            rest_copy(i, k).start()

    def share(i, owner):
        for k in range(1, n_rep):
            y_copy(i, owner, k).start()

    def from_outer(i):
        w = i // CUTS

        def hop(h, carry):
            @pl.when((depth >= h) & (depth >= low_depth(w)))
            def _():
                owner = fs - inward * h
                z_copy(i, owner, 0).wait_recv()
                z_copy(i, owner, 0).start()
                if spread:
                    pl.when((depth > 1) | (h > 1))(lambda: share(i, owner))
                else:
                    share(i, owner)

            return carry

        lax.fori_loop(1, (n_fs + 1) // 2, hop, 0)

    def from_inner(i, start, stop):
        w = i // CUTS

        def hop(h, carry):
            @pl.when((depth + h < n_fs) & (depth >= low_depth(w)))
            def _():
                owner = fs + inward * h
                z_copy(i, owner, 1).wait_recv()

                @pl.when(depth > low_depth(w))
                def _():
                    z_copy(i, owner, 1).start()

                share(i, owner)

            return carry

        lax.fori_loop(start, stop, hop, 0)

    def near(i):
        if i < items and n_fs > 1:
            from_inner(i, 1, 2)

    def early(i):
        from_outer(i)
        if i + AHEAD < items:
            when_busy(lambda: own(i + AHEAD))
        near(i + NEAR)

    def late(i):
        if n_fs > 2:
            from_inner(i, 2, n_fs)

    def arrived_one(w, owner):
        for cut in range(CUTS):
            i = w * CUTS + cut
            for k in range(1, n_rep):
                source = lax.rem(rep + n_rep - k, n_rep)
                ref = piece(i, owner, source)
                pltpu.make_async_remote_copy(
                    src_ref=ref, dst_ref=ref, send_sem=y_send.at[i, k - 1, owner],
                    recv_sem=y_recv.at[i, k - 1, owner],
                    device_id=at(source, fs, tp), device_id_type=MESH,
                ).wait_recv()

    def arrived(w):
        def one(h, carry):
            arrived_one(w, lax.rem(fs + h, n_fs))
            return carry

        lax.fori_loop(1, n_fs, one, 0)

    def sends_done():
        def one(owner, carry):
            offset = inward * (owner - fs)
            for i in range(items):
                low = low_depth(i // CUTS)
                if n_fs > 1:
                    passed = (offset == 0) | ((offset < 0) & (depth >= low))

                    @pl.when(passed)
                    def _():
                        z_copy(i, owner, 0).wait_send()

                @pl.when((offset >= 0) & (depth > low))
                def _():
                    z_copy(i, owner, 1).wait_send()

                sent = (offset != 0) & (depth >= low)
                if spread:
                    sent = sent & ((depth != 1) | (offset != -1))

                @pl.when(sent)
                def _():
                    for k in range(1, n_rep):
                        y_copy(i, owner, k).wait_send()

            return carry

        lax.fori_loop(0, n_fs, one, 0)

        def rest():
            for i in range(items):
                for k in range(1, n_rep):
                    rest_copy(i, k).wait_send()

        when_end(rest)

    def other_chip(k):
        return lax.rem(chip + k, n_chip)

    def source_chip(k):
        return lax.rem(chip + n_chip - k, n_chip)

    def tp_copy(src, dst, send, recv, target):
        return pltpu.make_async_remote_copy(
            src_ref=src, dst_ref=dst, send_sem=send, recv_sem=recv,
            device_id=at(rep, fs, target), device_id_type=MESH,
        )

    half = block // HALVES

    def gather_copy(phase, s, k, c):
        rows = pl.ds(pl.multiple_of(core * block + c * half, half), half)
        ref = rows_all.at[s, chip, rows]
        target = other_chip(k) * 2 + core
        return tp_copy(
            ref, ref, ag_sem.at[0, phase, s, k, c], ag_sem.at[1, phase, s, k, c], target
        )

    def pass_copy(phase, s, k):
        ref = rows_all.at[s, source_chip(k), mine]
        return tp_copy(ref, ref, agf_sem.at[0, phase, s, k], agf_sem.at[1, phase, s, k], sibling)

    def gather_send(phase, s, c):
        for k in range(1, n_chip):
            gather_copy(phase, s, k, c).start()

    def gather_start(phase, s, gain):
        rows_all[s, chip, mine] = norm_rows(resid[s].astype(jnp.float32), gain[...])
        gather_send(phase, s, 0)
        pass_copy(phase, s, 0).start()

    def gather_rest(phase, s):
        for c in range(1, HALVES):
            gather_send(phase, s, c)

    def gather_pass(phase, s):
        for k in range(1, n_chip):
            for c in range(HALVES):
                gather_copy(phase, s, k, c).wait_recv()
            pass_copy(phase, s, k).start()

    def gather_in(phase, s):
        for k in range(n_chip):
            pass_copy(phase, s, k).wait_recv()

    def gather_end(phase, s):
        for k in range(1, n_chip):
            for c in range(HALVES):
                gather_copy(phase, s, k, c).wait_send()
        for k in range(n_chip):
            pass_copy(phase, s, k).wait_send()

    def each_slot(run):
        def one(s, carry):
            run(s)
            return carry

        lax.fori_loop(low_slot, 2, one, 0)

    def each_pair(run):
        def one(p, carry):
            run(p)
            return carry

        lax.fori_loop(0, n_chip, one, 0)

    def sib_copy(s, p, f):
        return tp_copy(
            to_sibling.at[s, p, f], from_sibling.at[s, p, f],
            sib_sem.at[0, s, p, f], sib_sem.at[1, s, p, f], sibling,
        )

    def chip_copy(s, k, f):
        return tp_copy(
            to_chip.at[s, k - 1, f], from_chip.at[s, k - 1, f],
            chip_sem.at[0, s, k, f], chip_sem.at[1, s, k, f], other_chip(k) * 2 + core,
        )

    def product(s, p, f, left, w):
        part[...] = jnp.dot(left[s, p], full[w][f], preferred_element_type=jnp.float32)
        to_sibling[s, p, f] = part[theirs].astype(jnp.bfloat16)
        hold[s, p, f] = part[mine]
        sib_copy(s, p, f).start()

    def products(s, f, left, w):
        def one(k, carry):
            product(s, other_chip(k), f, left, w)
            return carry

        lax.fori_loop(1, n_chip + 1, one, 0)

    def joins(s, f):
        for k in range(1, n_chip):
            p = other_chip(k)
            sib_copy(s, p, f).wait_recv()
            joined = hold[s, p, f] + from_sibling[s, p, f].astype(jnp.float32)
            to_chip[s, k - 1, f] = joined.astype(jnp.bfloat16)
            chip_copy(s, k, f).start()

    def settle(s, f):
        sib_copy(s, chip, f).wait_recv()
        total = hold[s, chip, f] + from_sibling[s, chip, f].astype(jnp.float32)
        for k in range(1, n_chip):
            chip_copy(s, k, f).wait_recv()
            total = total + from_chip[s, k - 1, f].astype(jnp.float32)
        return total

    def reduce_end(s):
        def one(f, carry):
            for k in range(1, n_chip):
                chip_copy(s, k, f).wait_send()
            for p in range(n_chip):
                sib_copy(s, p, f).wait_send()
            return carry

        lax.fori_loop(0, n_fs, one, 0)

    def band(f):
        return slice(f * cols, (f + 1) * cols)

    def project(s, p, w):
        return jnp.dot(rows_all[s, p], full[w][...], preferred_element_type=jnp.float32)

    def gate_pair(s, p):
        gate_vals[s, p] = project(s, p, GATE)

    def lift_pair(s, p):
        hidden[s, p] = (jax.nn.silu(gate_vals[s, p]) * project(s, p, LIFT)).astype(jnp.bfloat16)

    def token_copy():
        return pltpu.make_async_remote_copy(
            src_ref=stream, dst_ref=resid.at[0], send_sem=token_sem.at[0],
            recv_sem=token_sem.at[1], device_id=at(rep, fs + inward, tp), device_id_type=MESH,
        )

    def second_copy(f):
        return pltpu.make_async_remote_copy(
            src_ref=resid.at[0, :, band(f)], dst_ref=resid.at[1, :, band(f)],
            send_sem=second_sem.at[0, f], recv_sem=second_sem.at[1, f],
            device_id=at(rep, fs - inward, tp), device_id_type=MESH,
        )

    def feed():
        token_copy().start()
        for i in range(items):
            own_end(i)

    when_end(feed)

    def open_own():
        for i in range(AHEAD):
            own(i)
        resid[1] = stream[...]
        gather_start(0, 1, gain_before)
        gather_rest(0, 1)

    when_busy(open_own)
    for i in range(NEAR):
        near(i)

    def open_guest():
        token_copy().wait_recv()
        gather_start(0, 0, gain_before)
        gather_rest(0, 0)

    def nth_owner(j):
        near = jnp.maximum(depth - j, 0) + j * jnp.minimum(jnp.maximum(j - depth, 0), 1)
        return near + side * (n_fs - 1 - 2 * near)

    def serve_all(w):
        for i in range(w * CUTS, (w + 1) * CUTS):
            serve(i)

    when_mid(open_guest)

    def gates():
        each_slot(lambda s: gather_in(0, s))
        arrived(GATE)
        each_slot(lambda s: each_pair(lambda p: gate_pair(s, p)))

    def lifts(s):
        each_pair(lambda p: lift_pair(s, p))
        gather_end(0, s)

    def lifts_own():
        arrived(LIFT)
        lifts(1)

    def down_block(owner):
        each_slot(lambda s: products(s, owner, hidden, DOWN))
        each_slot(lambda s: joins(s, owner))

    def downs(start, stop):
        def one(j, carry):
            owner = nth_owner(j)
            arrived_one(DOWN, owner)
            down_block(owner)
            return carry

        lax.fori_loop(start, stop, one, 0)

    def firsts():
        def one(s):
            for f in range(n_fs):
                base = resid[s, :, band(f)].astype(jnp.float32)
                resid[s, :, band(f)] = (base + 0.5 * settle(s, f)).astype(jnp.bfloat16)
            reduce_end(s)
            gather_start(1, s, mixer_gain)
            if spread:
                pl.when((s == 0) | (depth != 1))(lambda: gather_rest(1, s))
            else:
                gather_rest(1, s)

        each_slot(one)

    def guest_lifts():
        when_mid(lambda: lifts(0))
        when_busy(lambda: down_block(fs))

    stops = [1 + (n_fs - 1) * t // 3 for t in range(4)]
    first_down = MIX_U * CUTS
    between = {
        GATE * CUTS: lambda: when_busy(lambda: gather_pass(0, 1)),
        GATE * CUTS + 1: lambda: when_mid(lambda: gather_pass(0, 0)),
        LIFT * CUTS + 1: lambda: when_busy(gates),
        DOWN * CUTS: lambda: when_busy(lifts_own),
        DOWN * CUTS + 1: guest_lifts,
        first_down: lambda: when_busy(lambda: downs(stops[0], stops[1])),
        first_down + 1: lambda: when_busy(lambda: downs(stops[1], stops[2])),
        first_down + 2: lambda: when_busy(lambda: downs(stops[2], stops[3])),
        first_down + 3: lambda: when_busy(firsts),
    }
    for i in range(items):
        early(i)
        if i in between:
            between[i]()
        late(i)

    groups = spatial.shape[0]
    channels = lifted.shape[3]
    group_dim = channels // groups
    all_channels = channels * n_tp

    def u_pair(s, p):
        u_vals[s, p] = jax.nn.gelu(project(s, p, MIX_U))

    def v_pair(s, p):
        values = jax.nn.gelu(project(s, p, MIX_V))
        lifted[s, p] = values
        sums = jnp.sum(values, axis=1, keepdims=True)
        squares = jnp.sum(values * values, axis=1, keepdims=True)
        lane = lax.broadcasted_iota(jnp.int32, (pair, 128), 1)
        both = jnp.where(lane == 0, sums, jnp.where(lane == 1, squares, 0.0))
        mom_own[s, p] = both.T[:8]

    def mom_copy(s, k):
        return tp_copy(
            mom_own.at[s], mom_in.at[s, k - 1], mom_sem.at[0, s, k], mom_sem.at[1, s, k],
            lax.rem(tp + k, n_tp),
        )

    def values_of(s):
        gather_pass(1, s)
        gather_in(1, s)
        each_pair(lambda p: u_pair(s, p))
        each_pair(lambda p: v_pair(s, p))
        for k in range(1, n_tp):
            mom_copy(s, k).start()
        gather_end(1, s)

    def mix_of(s):
        for k in range(1, n_tp):
            mom_copy(s, k).wait_recv()
        shift_columns = square[...].T

        def mix_pair(p):
            moments = mom_own[s, p]
            for k in range(1, n_tp):
                moments = moments + mom_in[s, k - 1, p]
            moments = moments * (1.0 / all_channels)
            columns = jnp.concatenate([moments, jnp.zeros((120, pair), jnp.float32)], axis=0).T
            centre = columns[:, 0:1]
            spread_of = columns[:, 1:2] - centre * centre
            normed_v = (
                (lifted[s, p] - centre) * lax.rsqrt(spread_of + layer_epsilon) * layer_gain[...]
                + layer_shift[...]
            ).astype(jnp.bfloat16)
            for g in range(groups):
                cut = slice(g * group_dim, (g + 1) * group_dim)
                for b in range(pair // SPAN):
                    span = slice(b * SPAN, (b + 1) * SPAN)
                    mixed = jnp.dot(
                        masked[g], normed_v[span, cut], preferred_element_type=jnp.float32
                    )
                    mixed = mixed + shift_columns[:, g : g + 1]
                    gated[s, p, span, cut] = (u_vals[s, p, span, cut] * mixed).astype(jnp.bfloat16)

        each_pair(mix_pair)
        for k in range(1, n_tp):
            mom_copy(s, k).wait_send()

    def mixer_in():
        row = lax.broadcasted_iota(jnp.int32, (SPAN, SPAN), 0)
        col = lax.broadcasted_iota(jnp.int32, (SPAN, SPAN), 1)
        for g in range(groups):
            masked[g] = jnp.where(row >= col, spatial[g].astype(jnp.float32), 0.0).astype(
                jnp.bfloat16
            )
        square[...] = jnp.zeros_like(square)
        square[0:groups, :] = spatial_shift[...]
        arrived(MIX_U)
        arrived(MIX_V)

    when_busy(mixer_in)

    def span_of(s, start, stop):
        def over(run):
            def one(h, carry):
                run(lax.rem(fs + h, n_fs))
                return carry

            lax.fori_loop(start, stop, one, 0)

        over(lambda f: products(s, f, gated, MIX_DOWN))
        over(lambda f: joins(s, f))

    def mixer_out():
        middle = n_fs // 2

        def guest_in():
            values_of(0)
            gather_rest(1, 1)
            mix_of(0)
            arrived(MIX_DOWN)
            span_of(0, 0, middle)

        def guest_rest():
            span_of(0, middle, n_fs)

        when_mid(guest_in)
        values_of(1)
        if spread:
            pl.when(depth > 1)(lambda: arrived(MIX_DOWN))
        else:
            arrived(MIX_DOWN)
        when_mid(guest_rest)
        mix_of(1)
        span_of(1, 0, n_fs)

        def second(s, f):
            base = resid[s, :, band(f)].astype(jnp.float32)
            resid[s, :, band(f)] = (base + settle(s, f)).astype(jnp.bfloat16)

        def guest():
            for f in range(n_fs):
                second(0, f)
                second_copy(f).start()
            reduce_end(0)

        when_mid(guest)
        for f in range(n_fs):
            second(1, f)
        reduce_end(1)

    when_busy(mixer_out)

    def close_guest():
        arrived(GATE)
        arrived(LIFT)
        arrived(DOWN)
        for f in range(n_fs):
            second_copy(f).wait_recv()

    when_end(close_guest)
    def gather_half(k, c):
        ref = rows_last.at[chip, c, core]
        target = other_chip(k) * 2 + core
        return tp_copy(ref, ref, agl_sem.at[0, k, c], agl_sem.at[1, k, c], target)

    def pass_half(k, c):
        ref = rows_last.at[source_chip(k), c, core]
        return tp_copy(ref, ref, agl_sem.at[2, k, c], agl_sem.at[3, k, c], sibling)

    def sib_half(p, f, c):
        rows = pl.ds(c * half, half)
        return tp_copy(
            to_sibling.at[1, p, f, rows], from_sibling.at[1, p, f, rows],
            last_sem.at[0, p, f, c], last_sem.at[1, p, f, c], sibling,
        )

    def chip_half(k, f, c):
        rows = pl.ds(c * half, half)
        return tp_copy(
            to_chip.at[1, k - 1, f, rows], from_chip.at[1, k - 1, f, rows],
            last_sem.at[2, k, f, c], last_sem.at[3, k, f, c], other_chip(k) * 2 + core,
        )

    normed = norm_rows(resid[1].astype(jnp.float32), gain_after[...])
    for c in range(HALVES):
        rows_last[chip, c, core] = normed[c * half : (c + 1) * half]
        for k in range(1, n_chip):
            gather_half(k, c).start()
        pass_half(0, c).start()

    def last_rows(p, c):
        rows = rows_last[p, c].reshape(2 * half, width)
        gate = jnp.dot(rows, full[GATE][...], preferred_element_type=jnp.float32)
        lift = jnp.dot(rows, full[LIFT][...], preferred_element_type=jnp.float32)
        hidden_last[p, c] = (jax.nn.silu(gate) * lift).astype(jnp.bfloat16)

    def last_products(p, c):
        def one(f, carry):
            part_half[...] = jnp.dot(
                hidden_last[p, c], full[DOWN][f], preferred_element_type=jnp.float32
            ).reshape(part_half.shape)
            rows = pl.ds(c * half, half)
            to_sibling[1, p, f, rows] = part_half[1 - core].astype(jnp.bfloat16)
            hold[1, p, f, rows] = part_half[core]
            sib_half(p, f, c).start()
            return carry

        lax.fori_loop(0, n_fs, one, 0)

    def last_joins(k, c):
        p = other_chip(k)

        def one(f, carry):
            rows = pl.ds(c * half, half)
            sib_half(p, f, c).wait_recv()
            joined = hold[1, p, f, rows] + from_sibling[1, p, f, rows].astype(jnp.float32)
            to_chip[1, k - 1, f, rows] = joined.astype(jnp.bfloat16)
            chip_half(k, f, c).start()
            return carry

        lax.fori_loop(0, n_fs, one, 0)

    for c in range(HALVES):
        pass_half(0, c).wait_recv()
        last_rows(chip, c)
    for c in range(HALVES):
        for k in range(1, n_chip):
            gather_half(k, c).wait_recv()
            pass_half(k, c).start()
        for k in range(1, n_chip):
            pass_half(k, c).wait_recv()
            last_rows(other_chip(k), c)
            if c > 0:
                last_joins(k, c - 1)
            last_products(other_chip(k), c)
    last_products(chip, 0)
    for k in range(1, n_chip):
        last_joins(k, HALVES - 1)
    for c in range(1, HALVES):
        last_products(chip, c)
    for f in range(n_fs):
        for c in range(HALVES):
            sib_half(chip, f, c).wait_recv()
        total = hold[1, chip, f] + from_sibling[1, chip, f].astype(jnp.float32)
        for k in range(1, n_chip):
            for c in range(HALVES):
                chip_half(k, f, c).wait_recv()
            total = total + from_chip[1, k - 1, f].astype(jnp.float32)
        base = resid[1, :, band(f)].astype(jnp.float32)
        out[:, band(f)] = (base + 0.5 * total).astype(jnp.bfloat16)
    for c in range(HALVES):
        for k in range(n_chip):
            pass_half(k, c).wait_send()
        for k in range(1, n_chip):
            gather_half(k, c).wait_send()

    def last_sent(f, carry):
        for c in range(HALVES):
            for p in range(n_chip):
                sib_half(p, f, c).wait_send()
            for k in range(1, n_chip):
                chip_half(k, f, c).wait_send()
        return carry

    lax.fori_loop(0, n_fs, last_sent, 0)
    when_end(lambda: token_copy().wait_send())

    def shipped():
        for f in range(n_fs):
            second_copy(f).wait_send()

    when_mid(shipped)
    sends_done()


def body(
    n_rep,
    n_fs,
    n_tp,
    stream,
    gain_before,
    gain_after,
    proj_gate,
    proj_lift,
    proj_down,
    mixer_gain,
    mixer_u,
    mixer_v,
    layer_gain,
    layer_shift,
    spatial,
    spatial_shift,
    mixer_down,
):
    block, width = stream.shape
    n_chip = n_tp // 2
    pair = 2 * block
    cols = width // n_fs
    units = proj_gate.shape[1]
    channels = mixer_u.shape[1]
    bf16, f32 = jnp.bfloat16, jnp.float32
    shards = (proj_gate, proj_lift, proj_down, mixer_u, mixer_v, mixer_down)
    vmem = pl.BlockSpec(memory_space=pltpu.VMEM)
    anywhere = pl.BlockSpec(memory_space=pl.ANY)
    dma = pltpu.SemaphoreType.DMA
    spread_reps = max(n_rep - 1, 1)
    spread_chips = max(n_chip - 1, 1)
    return pl.pallas_call(
        functools.partial(layer_kernel, n_rep, n_fs, n_tp),
        out_shape=jax.ShapeDtypeStruct((block, width), bf16),
        in_specs=[vmem] * 8 + [anywhere] * 6,
        out_specs=vmem,
        scratch_shapes=[
            pltpu.VMEM(
                (n_fs * w.shape[0], w.shape[1]) if i in BY_ROWS else (n_fs,) + w.shape, bf16
            )
            for i, w in enumerate(shards)
        ]
        + [
            pltpu.VMEM((2, n_chip, pair, width), bf16),
            pltpu.VMEM((2, n_chip, n_fs, block, cols), bf16),
            pltpu.VMEM((2, n_chip, n_fs, block, cols), bf16),
            pltpu.VMEM((2, spread_chips, n_fs, block, cols), bf16),
            pltpu.VMEM((2, spread_chips, n_fs, block, cols), bf16),
            pltpu.VMEM((pair, cols), f32),
            pltpu.VMEM((2, n_chip, n_fs, block, cols), f32),
            pltpu.VMEM((2, n_chip, pair, units), f32),
            pltpu.VMEM((2, n_chip, pair, units), bf16),
            pltpu.VMEM((2, n_chip, pair, channels), f32),
            pltpu.VMEM((2, n_chip, pair, channels), f32),
            pltpu.VMEM((2, n_chip, pair, channels), bf16),
            pltpu.VMEM((n_chip, HALVES, 2, block // HALVES, width), bf16),
            pltpu.VMEM((n_chip, HALVES, 2 * block // HALVES, units), bf16),
            pltpu.VMEM((2, block // HALVES, cols), f32),
            pltpu.VMEM(spatial.shape, bf16),
            pltpu.VMEM((2, n_chip, 8, pair), f32),
            pltpu.VMEM((2, max(n_tp - 1, 1), n_chip, 8, pair), f32),
            pltpu.VMEM((128, SPAN), f32),
            pltpu.VMEM((2, block, width), bf16),
            dma((6,)),
            dma((2, 6 * CUTS, n_fs)),
            dma((6 * CUTS, n_fs)),
            dma((6 * CUTS, spread_reps, n_fs)),
            dma((6 * CUTS, spread_reps, n_fs)),
            dma((2, 2, 2, n_chip, HALVES)),
            dma((2, 2, 2, n_chip)),
            dma((2, 2, n_chip, n_fs)),
            dma((2, 2, n_chip, n_fs)),
            dma((2, 2, n_tp)),
            dma((2,)),
            dma((2, n_fs)),
            dma((4, n_chip, HALVES)),
            dma((4, n_chip, n_fs, HALVES)),
        ],
        compiler_params=pltpu.CompilerParams(
            collective_id=0, has_side_effects=True, vmem_limit_bytes=60 * 1024 * 1024
        ),
    )(
        stream,
        gain_before.reshape(1, -1),
        gain_after.reshape(1, -1),
        mixer_gain.reshape(1, -1),
        layer_gain.reshape(1, -1),
        layer_shift.reshape(1, -1),
        spatial,
        spatial_shift,
        *shards,
    )


def solution(mesh):
    placed = (
        P(("rep", "fs", "tp"), None),
        P(),
        P(),
        P("fs", "tp"),
        P("fs", "tp"),
        P("tp", "fs"),
        P(),
        P("fs", "tp"),
        P("fs", "tp"),
        P("tp"),
        P("tp"),
        P("tp", None, None),
        P("tp", None),
        P("tp", "fs"),
    )
    sizes = (mesh.shape["rep"], mesh.shape["fs"], mesh.shape["tp"])
    return jax.shard_map(
        functools.partial(body, *sizes),
        mesh=mesh,
        in_specs=placed,
        out_specs=P(("rep", "fs", "tp"), None),
        check_vma=False,
    )
```

```python
import functools

import jax
import jax.numpy as jnp
from jax import lax
from jax.experimental import pallas as pl
from jax.experimental.pallas import tpu as pltpu
from jax.sharding import PartitionSpec as P

SPAN = 128

norm_epsilon = 1e-06
layer_epsilon = 1e-05

MESH = pl.DeviceIdType.MESH
GATE, LIFT, DOWN, MIX_U, MIX_V, MIX_DOWN = range(6)
HALVES = 2
MIXERS = (MIX_U, MIX_V, MIX_DOWN)
BY_ROWS = (GATE, LIFT, MIX_U, MIX_V)


def cuts_of(shards, n_rep):
    return 2 if all(w.shape[0] % (n_rep * 32) == 0 for w in shards) else 1


def norm_rows(widened, scale_gain):
    factor = lax.rsqrt(jnp.mean(widened * widened, axis=1, keepdims=True) + norm_epsilon)
    return (widened * factor * scale_gain).astype(jnp.bfloat16)


def layer_kernel(
    n_rep,
    n_fs,
    n_tp,
    stream,
    gain_before,
    gain_after,
    mixer_gain,
    layer_gain,
    layer_shift,
    spatial,
    spatial_shift,
    proj_gate,
    proj_lift,
    proj_down,
    mixer_u,
    mixer_v,
    mixer_down,
    out,
    gate_all,
    lift_all,
    down_all,
    u_all,
    v_all,
    mix_down_all,
    rows_all,
    to_sibling,
    from_sibling,
    to_chip,
    from_chip,
    part,
    hold,
    gate_vals,
    hidden,
    u_vals,
    lifted,
    gated,
    rows_last,
    hidden_last,
    part_half,
    masked,
    mom_own,
    mom_in,
    square,
    resid,
    local_sem,
    z_send,
    z_recv,
    y_send,
    y_recv,
    ag_sem,
    agf_sem,
    sib_sem,
    chip_sem,
    mom_sem,
    token_sem,
    second_sem,
    agl_sem,
    last_sem,
):
    rep, fs, tp = lax.axis_index("rep"), lax.axis_index("fs"), lax.axis_index("tp")
    chip, core = tp // 2, lax.rem(tp, 2)
    n_chip = n_tp // 2
    block, width = stream.shape
    pair = 2 * block
    cols = width // n_fs
    shards = (proj_gate, proj_lift, proj_down, mixer_u, mixer_v, mixer_down)
    cuts = cuts_of(shards, n_rep)
    ahead, near_by = cuts + 2, cuts
    full = (gate_all, lift_all, down_all, u_all, v_all, mix_down_all)
    mine = pl.ds(pl.multiple_of(core * block, block), block)
    theirs = pl.ds(pl.multiple_of((1 - core) * block, block), block)
    sibling = chip * 2 + (1 - core)

    spread = n_fs >= 4
    depth = jnp.minimum(fs, n_fs - 1 - fs)
    side = (2 * fs) // n_fs
    inward = 1 - 2 * side
    if spread:
        low_slot = lax.rem(jnp.minimum(depth, 2) + 2, 3)
        at_end, at_mid = depth == 0, depth == 1
    else:
        low_slot = 1
    busy = low_slot < 2

    def when_busy(run):
        if spread:
            pl.when(busy)(run)
        else:
            run()

    def when_mid(run):
        if spread:
            pl.when(at_mid)(run)

    def when_end(run):
        if spread:
            pl.when(at_end)(run)

    def low_depth(w):
        return 1 if spread and w in MIXERS else 0

    def at(r, f, t):
        return (r, f, t)

    barrier = pltpu.get_barrier_semaphore()

    @pl.when(fs > 0)
    def _():
        pl.semaphore_signal(barrier, inc=1, device_id=at(rep, fs - 1, tp), device_id_type=MESH)

    @pl.when(fs < n_fs - 1)
    def _():
        pl.semaphore_signal(barrier, inc=1, device_id=at(rep, fs + 1, tp), device_id_type=MESH)

    for k in range(1, n_rep):
        pl.semaphore_signal(
            barrier, inc=1, device_id=at(lax.rem(rep + k, n_rep), fs, tp), device_id_type=MESH
        )
    for k in range(1, n_tp):
        pl.semaphore_signal(
            barrier, inc=1, device_id=at(rep, fs, lax.rem(tp + k, n_tp)), device_id_type=MESH
        )

    def depth_of(w):
        return shards[w].shape[0]

    def whole(w, owner):
        if w in BY_ROWS:
            n = depth_of(w)
            return full[w].at[pl.ds(pl.multiple_of(owner * n, n), n)]
        return full[w].at[owner]

    locals_ = [
        pltpu.make_async_copy(shards[w], whole(w, fs), local_sem.at[w]) for w in range(6)
    ]
    for copy in locals_:
        copy.start()

    line_peers = jnp.minimum(fs, 1) + jnp.minimum(n_fs - 1 - fs, 1)
    pl.semaphore_wait(barrier, n_rep - 1 + n_tp - 1 + line_peers)

    items = 6 * cuts

    def piece(i, owner, part_index):
        w, cut = i // cuts, i % cuts
        rows = depth_of(w) // (n_rep * cuts)
        first_row = (part_index * cuts + cut) * rows
        if w in BY_ROWS:
            start = pl.multiple_of(owner * depth_of(w) + first_row, rows)
            return full[w].at[pl.ds(start, rows)]
        return full[w].at[owner, pl.ds(pl.multiple_of(first_row, rows), rows)]

    def z_copy(i, owner, out):
        ref = piece(i, owner, rep)
        step = inward if out == 0 else -inward
        return pltpu.make_async_remote_copy(
            src_ref=ref, dst_ref=ref, send_sem=z_send.at[out, i, owner],
            recv_sem=z_recv.at[i, owner],
            device_id=at(rep, fs + step, tp), device_id_type=MESH,
        )

    def rest_copy(i, k):
        ref = piece(i, fs, lax.rem(rep + n_rep - k, n_rep))
        return pltpu.make_async_remote_copy(
            src_ref=ref, dst_ref=ref, send_sem=y_send.at[i, k - 1, fs],
            recv_sem=y_recv.at[i, k - 1, fs],
            device_id=at(rep, fs + inward, tp), device_id_type=MESH,
        )

    def y_copy(i, owner, k):
        ref = piece(i, owner, rep)
        return pltpu.make_async_remote_copy(
            src_ref=ref, dst_ref=ref, send_sem=y_send.at[i, k - 1, owner],
            recv_sem=y_recv.at[i, k - 1, owner],
            device_id=at(lax.rem(rep + k, n_rep), fs, tp), device_id_type=MESH,
        )

    def own(i):
        w = i // cuts
        if i % cuts == 0:
            locals_[w].wait()
        if n_fs > 1:
            z_copy(i, fs, 0).start()

        @pl.when(depth > low_depth(w))
        def _():
            z_copy(i, fs, 1).start()

    def rest_end(i):
        for k in range(1, n_rep):
            rest_copy(i, k).start()

    def share(i, owner):
        for k in range(1, n_rep):
            y_copy(i, owner, k).start()

    def from_outer(i):
        w = i // cuts

        def hop(h, carry):
            @pl.when((depth >= h) & (depth >= low_depth(w)))
            def _():
                owner = fs - inward * h
                z_copy(i, owner, 0).wait_recv()
                z_copy(i, owner, 0).start()
                if spread:
                    pl.when((depth > 1) | (h > 1))(lambda: share(i, owner))
                else:
                    share(i, owner)

            return carry

        lax.fori_loop(1, (n_fs + 1) // 2, hop, 0)

    def from_inner(i, start, stop):
        w = i // cuts

        def hop(h, carry):
            @pl.when((depth + h < n_fs) & (depth >= low_depth(w)))
            def _():
                owner = fs + inward * h
                z_copy(i, owner, 1).wait_recv()

                @pl.when(depth > low_depth(w))
                def _():
                    z_copy(i, owner, 1).start()

                share(i, owner)

            return carry

        lax.fori_loop(start, stop, hop, 0)

    def near(i):
        if i < items and n_fs > 1:
            from_inner(i, 1, 2)

    def early(i):
        from_outer(i)
        if i < MIX_U * cuts - near_by:
            near(i + near_by)
        elif i >= MIX_U * cuts - 1:
            near(i + 1)

    def late(i):
        if n_fs > 2:
            from_inner(i, 2, n_fs)
        if i + ahead < items:
            when_busy(lambda: own(i + ahead))

    def arrived_one(w, owner):
        for cut in range(cuts):
            i = w * cuts + cut
            for k in range(1, n_rep):
                source = lax.rem(rep + n_rep - k, n_rep)
                ref = piece(i, owner, source)
                pltpu.make_async_remote_copy(
                    src_ref=ref, dst_ref=ref, send_sem=y_send.at[i, k - 1, owner],
                    recv_sem=y_recv.at[i, k - 1, owner],
                    device_id=at(source, fs, tp), device_id_type=MESH,
                ).wait_recv()

    def arrived(w):
        def one(h, carry):
            arrived_one(w, lax.rem(fs + h, n_fs))
            return carry

        lax.fori_loop(1, n_fs, one, 0)

    def sends_done():
        def one(owner, carry):
            offset = inward * (owner - fs)
            for i in range(items):
                low = low_depth(i // cuts)
                if n_fs > 1:
                    passed = (offset == 0) | ((offset < 0) & (depth >= low))

                    @pl.when(passed)
                    def _():
                        z_copy(i, owner, 0).wait_send()

                @pl.when((offset >= 0) & (depth > low))
                def _():
                    z_copy(i, owner, 1).wait_send()

                sent = (offset != 0) & (depth >= low)
                if spread:
                    sent = sent & ((depth != 1) | (offset != -1))

                @pl.when(sent)
                def _():
                    for k in range(1, n_rep):
                        y_copy(i, owner, k).wait_send()

            return carry

        lax.fori_loop(0, n_fs, one, 0)

        def rest():
            for i in range(items):
                for k in range(1, n_rep):
                    rest_copy(i, k).wait_send()

        when_end(rest)

    def other_chip(k):
        return lax.rem(chip + k, n_chip)

    def source_chip(k):
        return lax.rem(chip + n_chip - k, n_chip)

    def tp_copy(src, dst, send, recv, target):
        return pltpu.make_async_remote_copy(
            src_ref=src, dst_ref=dst, send_sem=send, recv_sem=recv,
            device_id=at(rep, fs, target), device_id_type=MESH,
        )

    half = block // HALVES

    def gather_copy(phase, s, k, c):
        rows = pl.ds(pl.multiple_of(core * block + c * half, half), half)
        ref = rows_all.at[s, chip, rows]
        target = other_chip(k) * 2 + core
        return tp_copy(
            ref, ref, ag_sem.at[0, phase, s, k, c], ag_sem.at[1, phase, s, k, c], target
        )

    def pass_copy(phase, s, k):
        ref = rows_all.at[s, source_chip(k), mine]
        return tp_copy(ref, ref, agf_sem.at[0, phase, s, k], agf_sem.at[1, phase, s, k], sibling)

    def gather_send(phase, s, c):
        for k in range(1, n_chip):
            gather_copy(phase, s, k, c).start()

    def gather_start(phase, s, gain):
        rows_all[s, chip, mine] = norm_rows(resid[s].astype(jnp.float32), gain[...])
        gather_send(phase, s, 0)
        pass_copy(phase, s, 0).start()

    def gather_rest(phase, s):
        for c in range(1, HALVES):
            gather_send(phase, s, c)

    def gather_pass(phase, s):
        for k in range(1, n_chip):
            for c in range(HALVES):
                gather_copy(phase, s, k, c).wait_recv()
            pass_copy(phase, s, k).start()

    def gather_in(phase, s):
        for k in range(n_chip):
            pass_copy(phase, s, k).wait_recv()

    def gather_end(phase, s):
        for k in range(1, n_chip):
            for c in range(HALVES):
                gather_copy(phase, s, k, c).wait_send()
        for k in range(n_chip):
            pass_copy(phase, s, k).wait_send()

    def each_slot(run):
        def one(s, carry):
            run(s)
            return carry

        lax.fori_loop(low_slot, 2, one, 0)

    def each_pair(run):
        def one(p, carry):
            run(p)
            return carry

        lax.fori_loop(0, n_chip, one, 0)

    def sib_copy(s, p, f):
        return tp_copy(
            to_sibling.at[s, p, f], from_sibling.at[s, p, f],
            sib_sem.at[0, s, p, f], sib_sem.at[1, s, p, f], sibling,
        )

    def chip_copy(s, k, f):
        return tp_copy(
            to_chip.at[s, k - 1, f], from_chip.at[s, k - 1, f],
            chip_sem.at[0, s, k, f], chip_sem.at[1, s, k, f], other_chip(k) * 2 + core,
        )

    def product(s, p, f, left, w):
        part[...] = jnp.dot(left[s, p], full[w][f], preferred_element_type=jnp.float32)
        to_sibling[s, p, f] = part[theirs].astype(jnp.bfloat16)
        hold[s, p, f] = part[mine]
        sib_copy(s, p, f).start()

    def products(s, f, left, w):
        def one(k, carry):
            product(s, other_chip(k), f, left, w)
            return carry

        lax.fori_loop(1, n_chip + 1, one, 0)

    def joins(s, f):
        for k in range(1, n_chip):
            p = other_chip(k)
            sib_copy(s, p, f).wait_recv()
            joined = hold[s, p, f] + from_sibling[s, p, f].astype(jnp.float32)
            to_chip[s, k - 1, f] = joined.astype(jnp.bfloat16)
            chip_copy(s, k, f).start()

    def settle(s, f):
        sib_copy(s, chip, f).wait_recv()
        total = hold[s, chip, f] + from_sibling[s, chip, f].astype(jnp.float32)
        for k in range(1, n_chip):
            chip_copy(s, k, f).wait_recv()
            total = total + from_chip[s, k - 1, f].astype(jnp.float32)
        return total

    def reduce_end(s):
        def one(f, carry):
            for k in range(1, n_chip):
                chip_copy(s, k, f).wait_send()
            for p in range(n_chip):
                sib_copy(s, p, f).wait_send()
            return carry

        lax.fori_loop(0, n_fs, one, 0)

    def band(f):
        return pl.ds(pl.multiple_of(f * cols, cols), cols)

    def project(s, p, w):
        return jnp.dot(rows_all[s, p], full[w][...], preferred_element_type=jnp.float32)

    def gate_pair(s, p):
        gate_vals[s, p] = project(s, p, GATE)

    def lift_pair(s, p):
        hidden[s, p] = (jax.nn.silu(gate_vals[s, p]) * project(s, p, LIFT)).astype(jnp.bfloat16)

    def token_copy():
        return pltpu.make_async_remote_copy(
            src_ref=stream, dst_ref=resid.at[0], send_sem=token_sem.at[0],
            recv_sem=token_sem.at[1], device_id=at(rep, fs + inward, tp), device_id_type=MESH,
        )

    def second_copy(f):
        return pltpu.make_async_remote_copy(
            src_ref=resid.at[0, :, band(f)], dst_ref=resid.at[1, :, band(f)],
            send_sem=second_sem.at[0, f], recv_sem=second_sem.at[1, f],
            device_id=at(rep, fs - inward, tp), device_id_type=MESH,
        )

    def feed():
        token_copy().start()
        for w in range(6):
            for i in range(w * cuts, (w + 1) * cuts):
                own(i)
            for i in range(w * cuts, (w + 1) * cuts):
                rest_end(i)

    when_end(feed)

    def open_own():
        for i in range(ahead):
            own(i)
        resid[1] = stream[...]
        gather_start(0, 1, gain_before)
        gather_rest(0, 1)

    when_busy(open_own)
    for i in range(near_by):
        near(i)

    def open_guest():
        token_copy().wait_recv()
        gather_start(0, 0, gain_before)
        gather_rest(0, 0)

    def nth_owner(j):
        beyond = jnp.maximum(j - 1, 0)
        outs = jnp.minimum(beyond, depth)
        ins = beyond - outs
        first, far = jnp.minimum(beyond, 1), jnp.minimum(ins, 1)
        offset = (1 - first) * jnp.minimum(j, 1) + far * (ins + 1) - (first - far) * outs
        return fs + inward * offset

    when_mid(open_guest)

    def gates():
        each_slot(lambda s: gather_in(0, s))
        arrived(GATE)
        each_slot(lambda s: each_pair(lambda p: gate_pair(s, p)))

    def lifts(s):
        each_pair(lambda p: lift_pair(s, p))
        gather_end(0, s)

    def lifts_own():
        arrived(LIFT)
        lifts(1)
        products(1, fs, hidden, DOWN)
        joins(1, fs)

    def down_block(owner):
        each_slot(lambda s: products(s, owner, hidden, DOWN))
        each_slot(lambda s: joins(s, owner))

    def downs(start, stop):
        def one(j, carry):
            owner = nth_owner(j)
            arrived_one(DOWN, owner)
            down_block(owner)
            return carry

        lax.fori_loop(start, stop, one, 0)

    def first_band(s, j):
        f = nth_owner(j)
        base = resid[s, :, band(f)].astype(jnp.float32)
        resid[s, :, band(f)] = (base + 0.5 * settle(s, f)).astype(jnp.bfloat16)

    def first_bands(s, start, stop):
        def one(j, carry):
            first_band(s, j)
            return carry

        lax.fori_loop(start, stop, one, 0)

    def last_downs():
        downs(stops[2], stops[3])
        each_slot(lambda s: first_bands(s, 0, n_fs - 1))

    def first_of(s):
        first_bands(s, n_fs - 1, n_fs)
        gather_start(1, s, mixer_gain)

    def guest_first():
        first_of(0)
        gather_rest(1, 0)

    def own_first():
        first_of(1)
        if spread:
            pl.when(depth != 1)(lambda: gather_rest(1, 1))
        else:
            gather_rest(1, 1)
        each_slot(reduce_end)

    def guest_lifts():
        lifts(0)
        products(0, fs, hidden, DOWN)
        joins(0, fs)

    stops = [1 + (n_fs - 1) * t // 3 for t in range(4)]

    def far_downs():
        downs(stops[2], stops[3])
        each_slot(lambda s: first_bands(s, 0, n_fs - 1))

    groups = spatial.shape[0]
    channels = lifted.shape[3]
    group_dim = channels // groups
    all_channels = channels * n_tp

    def u_pair(s, p):
        u_vals[s, p] = jax.nn.gelu(project(s, p, MIX_U))

    def v_pair(s, p):
        values = jax.nn.gelu(project(s, p, MIX_V))
        lifted[s, p] = values
        sums = jnp.sum(values, axis=1, keepdims=True)
        squares = jnp.sum(values * values, axis=1, keepdims=True)
        lane = lax.broadcasted_iota(jnp.int32, (pair, 128), 1)
        both = jnp.where(lane == 0, sums, jnp.where(lane == 1, squares, 0.0))
        mom_own[s, p] = both.T[:8]

    def mom_copy(s, k):
        return tp_copy(
            mom_own.at[s], mom_in.at[s, k - 1], mom_sem.at[0, s, k], mom_sem.at[1, s, k],
            lax.rem(tp + k, n_tp),
        )

    def values_of(s):
        gather_pass(1, s)
        gather_in(1, s)
        each_pair(lambda p: u_pair(s, p))
        each_pair(lambda p: v_pair(s, p))
        for k in range(1, n_tp):
            mom_copy(s, k).start()
        gather_end(1, s)

    def mix_of(s):
        for k in range(1, n_tp):
            mom_copy(s, k).wait_recv()
        shift_columns = square[...].T

        def mix_pair(p):
            moments = mom_own[s, p]
            for k in range(1, n_tp):
                moments = moments + mom_in[s, k - 1, p]
            moments = moments * (1.0 / all_channels)
            columns = jnp.concatenate([moments, jnp.zeros((120, pair), jnp.float32)], axis=0).T
            centre = columns[:, 0:1]
            spread_of = columns[:, 1:2] - centre * centre
            normed_v = (
                (lifted[s, p] - centre) * lax.rsqrt(spread_of + layer_epsilon) * layer_gain[...]
                + layer_shift[...]
            ).astype(jnp.bfloat16)
            for g in range(groups):
                cut = slice(g * group_dim, (g + 1) * group_dim)
                for b in range(pair // SPAN):
                    span = slice(b * SPAN, (b + 1) * SPAN)
                    mixed = jnp.dot(
                        masked[g], normed_v[span, cut], preferred_element_type=jnp.float32
                    )
                    mixed = mixed + shift_columns[:, g : g + 1]
                    gated[s, p, span, cut] = (u_vals[s, p, span, cut] * mixed).astype(jnp.bfloat16)

        each_pair(mix_pair)
        for k in range(1, n_tp):
            mom_copy(s, k).wait_send()

    def guest_values():
        values_of(0)
        gather_rest(1, 1)

    def mixer_in():
        row = lax.broadcasted_iota(jnp.int32, (SPAN, SPAN), 0)
        col = lax.broadcasted_iota(jnp.int32, (SPAN, SPAN), 1)
        for g in range(groups):
            masked[g] = jnp.where(row >= col, spatial[g].astype(jnp.float32), 0.0).astype(
                jnp.bfloat16
            )
        square[...] = jnp.zeros_like(square)
        square[0:groups, :] = spatial_shift[...]
        arrived(MIX_U)
        arrived(MIX_V)
        when_mid(guest_values)


    between = {
        (GATE, 0): lambda: when_busy(lambda: gather_pass(0, 1)),
        (GATE, 3): lambda: when_mid(lambda: gather_pass(0, 0)),
        (LIFT, 2): lambda: when_busy(gates),
        (DOWN, 0): lambda: when_busy(lifts_own),
        (DOWN, 1): lambda: when_mid(guest_lifts),
        (DOWN, 2): lambda: when_busy(lambda: downs(stops[0], stops[1])),
        (DOWN, 3): lambda: when_busy(lambda: downs(stops[1], stops[2])),
        (MIX_U, 1): lambda: when_busy(far_downs),
        (MIX_U, 3): lambda: when_mid(guest_first),
        (MIX_V, 1): lambda: when_busy(own_first),
        (MIX_DOWN, 1): lambda: when_busy(mixer_in),
    }
    for w in range(6):
        for stage, step in enumerate((early, late)):
            for i in range(w * cuts, (w + 1) * cuts):
                step(i)
                for place, edge in enumerate((w * cuts, (w + 1) * cuts - 1)):
                    if i == edge and (w, 2 * stage + place) in between:
                        between[w, 2 * stage + place]()

    def bands_of(start, stop, run):
        def one(h, carry):
            run(lax.rem(fs + h, n_fs))
            return carry

        lax.fori_loop(start, stop, one, 0)

    def span_of(s, start, stop):
        bands_of(start, stop, lambda f: products(s, f, gated, MIX_DOWN))
        bands_of(start, stop, lambda f: joins(s, f))

    def second_band(s, f):
        base = resid[s, :, band(f)].astype(jnp.float32)
        resid[s, :, band(f)] = (base + settle(s, f)).astype(jnp.bfloat16)

    def ship(start, stop):
        def one(f):
            second_band(0, f)
            second_copy(f).start()

        bands_of(start, stop, one)

    def mixer_out():
        middle = n_fs // 2

        def guest_in():
            mix_of(0)
            arrived(MIX_DOWN)
            span_of(0, 0, middle)

        def guest_rest():
            span_of(0, middle, n_fs)
            ship(0, middle)

        def guest_ship():
            ship(middle, n_fs)
            reduce_end(0)

        when_mid(guest_in)
        values_of(1)
        if spread:
            pl.when(depth > 1)(lambda: arrived(MIX_DOWN))
        else:
            arrived(MIX_DOWN)
        when_mid(guest_rest)
        mix_of(1)
        span_of(1, 0, n_fs)
        when_mid(guest_ship)
        bands_of(0, n_fs, lambda f: second_band(1, f))
        reduce_end(1)

    when_busy(mixer_out)

    def close_guest():
        arrived(GATE)
        arrived(LIFT)
        arrived(DOWN)
        for f in range(n_fs):
            second_copy(f).wait_recv()

    when_end(close_guest)
    def gather_half(k, c):
        ref = rows_last.at[chip, c, core]
        target = other_chip(k) * 2 + core
        return tp_copy(ref, ref, agl_sem.at[0, k, c], agl_sem.at[1, k, c], target)

    def pass_half(k, c):
        ref = rows_last.at[source_chip(k), c, core]
        return tp_copy(ref, ref, agl_sem.at[2, k, c], agl_sem.at[3, k, c], sibling)

    def sib_half(p, f, c):
        rows = pl.ds(c * half, half)
        return tp_copy(
            to_sibling.at[1, p, f, rows], from_sibling.at[1, p, f, rows],
            last_sem.at[0, p, f, c], last_sem.at[1, p, f, c], sibling,
        )

    def chip_half(k, f, c):
        rows = pl.ds(c * half, half)
        return tp_copy(
            to_chip.at[1, k - 1, f, rows], from_chip.at[1, k - 1, f, rows],
            last_sem.at[2, k, f, c], last_sem.at[3, k, f, c], other_chip(k) * 2 + core,
        )

    normed = norm_rows(resid[1].astype(jnp.float32), gain_after[...])
    for c in range(HALVES):
        rows_last[chip, c, core] = normed[c * half : (c + 1) * half]
        for k in range(1, n_chip):
            gather_half(k, c).start()
        pass_half(0, c).start()

    def last_rows(p, c):
        rows = rows_last[p, c].reshape(2 * half, width)
        gate = jnp.dot(rows, full[GATE][...], preferred_element_type=jnp.float32)
        lift = jnp.dot(rows, full[LIFT][...], preferred_element_type=jnp.float32)
        hidden_last[p, c] = (jax.nn.silu(gate) * lift).astype(jnp.bfloat16)

    def last_products(p, c):
        def one(f, carry):
            part_half[...] = jnp.dot(
                hidden_last[p, c], full[DOWN][f], preferred_element_type=jnp.float32
            ).reshape(part_half.shape)
            rows = pl.ds(c * half, half)
            to_sibling[1, p, f, rows] = part_half[1 - core].astype(jnp.bfloat16)
            hold[1, p, f, rows] = part_half[core]
            sib_half(p, f, c).start()
            return carry

        lax.fori_loop(0, n_fs, one, 0)

    def last_joins(k, c):
        p = other_chip(k)

        def one(f, carry):
            rows = pl.ds(c * half, half)
            sib_half(p, f, c).wait_recv()
            joined = hold[1, p, f, rows] + from_sibling[1, p, f, rows].astype(jnp.float32)
            to_chip[1, k - 1, f, rows] = joined.astype(jnp.bfloat16)
            chip_half(k, f, c).start()
            return carry

        lax.fori_loop(0, n_fs, one, 0)

    for c in range(HALVES):
        pass_half(0, c).wait_recv()
        last_rows(chip, c)
    for c in range(HALVES):
        for k in range(1, n_chip):
            gather_half(k, c).wait_recv()
            pass_half(k, c).start()
        for k in range(1, n_chip):
            pass_half(k, c).wait_recv()
            last_rows(other_chip(k), c)
            last_products(other_chip(k), c)
        last_products(chip, c)
        for k in range(1, n_chip):
            last_joins(k, c)
    for f in range(n_fs):
        for c in range(HALVES):
            sib_half(chip, f, c).wait_recv()
        total = hold[1, chip, f] + from_sibling[1, chip, f].astype(jnp.float32)
        for k in range(1, n_chip):
            for c in range(HALVES):
                chip_half(k, f, c).wait_recv()
            total = total + from_chip[1, k - 1, f].astype(jnp.float32)
        base = resid[1, :, band(f)].astype(jnp.float32)
        out[:, band(f)] = (base + 0.5 * total).astype(jnp.bfloat16)
    for c in range(HALVES):
        for k in range(n_chip):
            pass_half(k, c).wait_send()
        for k in range(1, n_chip):
            gather_half(k, c).wait_send()

    def last_sent(f, carry):
        for c in range(HALVES):
            for p in range(n_chip):
                sib_half(p, f, c).wait_send()
            for k in range(1, n_chip):
                chip_half(k, f, c).wait_send()
        return carry

    lax.fori_loop(0, n_fs, last_sent, 0)
    when_end(lambda: token_copy().wait_send())

    def shipped():
        for f in range(n_fs):
            second_copy(f).wait_send()

    when_mid(shipped)
    sends_done()


def body(
    n_rep,
    n_fs,
    n_tp,
    stream,
    gain_before,
    gain_after,
    proj_gate,
    proj_lift,
    proj_down,
    mixer_gain,
    mixer_u,
    mixer_v,
    layer_gain,
    layer_shift,
    spatial,
    spatial_shift,
    mixer_down,
):
    block, width = stream.shape
    n_chip = n_tp // 2
    pair = 2 * block
    cols = width // n_fs
    units = proj_gate.shape[1]
    channels = mixer_u.shape[1]
    bf16, f32 = jnp.bfloat16, jnp.float32
    shards = (proj_gate, proj_lift, proj_down, mixer_u, mixer_v, mixer_down)
    cuts = cuts_of(shards, n_rep)
    vmem = pl.BlockSpec(memory_space=pltpu.VMEM)
    anywhere = pl.BlockSpec(memory_space=pl.ANY)
    dma = pltpu.SemaphoreType.DMA
    spread_reps = max(n_rep - 1, 1)
    spread_chips = max(n_chip - 1, 1)
    return pl.pallas_call(
        functools.partial(layer_kernel, n_rep, n_fs, n_tp),
        out_shape=pltpu.VMEM((block, width), bf16),
        in_specs=[vmem] * 8 + [anywhere] * 6,
        out_specs=vmem,
        scratch_shapes=[
            pltpu.VMEM(
                (n_fs * w.shape[0], w.shape[1]) if i in BY_ROWS else (n_fs,) + w.shape, bf16
            )
            for i, w in enumerate(shards)
        ]
        + [
            pltpu.VMEM((2, n_chip, pair, width), bf16),
            pltpu.VMEM((2, n_chip, n_fs, block, cols), bf16),
            pltpu.VMEM((2, n_chip, n_fs, block, cols), bf16),
            pltpu.VMEM((2, spread_chips, n_fs, block, cols), bf16),
            pltpu.VMEM((2, spread_chips, n_fs, block, cols), bf16),
            pltpu.VMEM((pair, cols), f32),
            pltpu.VMEM((2, n_chip, n_fs, block, cols), f32),
            pltpu.VMEM((2, n_chip, pair, units), f32),
            pltpu.VMEM((2, n_chip, pair, units), bf16),
            pltpu.VMEM((2, n_chip, pair, channels), f32),
            pltpu.VMEM((2, n_chip, pair, channels), f32),
            pltpu.VMEM((2, n_chip, pair, channels), bf16),
            pltpu.VMEM((n_chip, HALVES, 2, block // HALVES, width), bf16),
            pltpu.VMEM((n_chip, HALVES, 2 * block // HALVES, units), bf16),
            pltpu.VMEM((2, block // HALVES, cols), f32),
            pltpu.VMEM(spatial.shape, bf16),
            pltpu.VMEM((2, n_chip, 8, pair), f32),
            pltpu.VMEM((2, max(n_tp - 1, 1), n_chip, 8, pair), f32),
            pltpu.VMEM((128, SPAN), f32),
            pltpu.VMEM((2, block, width), bf16),
            dma((6,)),
            dma((2, 6 * cuts, n_fs)),
            dma((6 * cuts, n_fs)),
            dma((6 * cuts, spread_reps, n_fs)),
            dma((6 * cuts, spread_reps, n_fs)),
            dma((2, 2, 2, n_chip, HALVES)),
            dma((2, 2, 2, n_chip)),
            dma((2, 2, n_chip, n_fs)),
            dma((2, 2, n_chip, n_fs)),
            dma((2, 2, n_tp)),
            dma((2,)),
            dma((2, n_fs)),
            dma((4, n_chip, HALVES)),
            dma((4, n_chip, n_fs, HALVES)),
        ],
        compiler_params=pltpu.CompilerParams(
            collective_id=0, has_side_effects=True, vmem_limit_bytes=60 * 1024 * 1024
        ),
    )(
        stream,
        gain_before.reshape(1, -1),
        gain_after.reshape(1, -1),
        mixer_gain.reshape(1, -1),
        layer_gain.reshape(1, -1),
        layer_shift.reshape(1, -1),
        spatial,
        spatial_shift,
        *shards,
    )


def solution(mesh):
    placed = (
        P(("rep", "fs", "tp"), None),
        P(),
        P(),
        P("fs", "tp"),
        P("fs", "tp"),
        P("tp", "fs"),
        P(),
        P("fs", "tp"),
        P("fs", "tp"),
        P("tp"),
        P("tp"),
        P("tp", None, None),
        P("tp", None),
        P("tp", "fs"),
    )
    sizes = (mesh.shape["rep"], mesh.shape["fs"], mesh.shape["tp"])
    return jax.shard_map(
        functools.partial(body, *sizes),
        mesh=mesh,
        in_specs=placed,
        out_specs=P(("rep", "fs", "tp"), None),
        check_vma=False,
    )
```

```python
import functools

import jax
import jax.numpy as jnp
from jax import lax
from jax.experimental import pallas as pl
from jax.experimental.pallas import tpu as pltpu
from jax.sharding import PartitionSpec as P

SPAN = 128

norm_epsilon = 1e-06
layer_epsilon = 1e-05

MESH = pl.DeviceIdType.MESH
GATE, LIFT, DOWN, MIX_U, MIX_V, MIX_DOWN = range(6)
HALVES = 2
MIXERS = (MIX_U, MIX_V, MIX_DOWN)
BY_ROWS = (GATE, LIFT, MIX_U, MIX_V)


def cuts_of(shards, n_rep):
    return 2 if all(w.shape[0] % (n_rep * 32) == 0 for w in shards) else 1


def norm_rows(widened, scale_gain):
    factor = lax.rsqrt(jnp.mean(widened * widened, axis=1, keepdims=True) + norm_epsilon)
    return (widened * factor * scale_gain).astype(jnp.bfloat16)


def layer_kernel(
    n_rep,
    n_fs,
    n_tp,
    stream,
    gain_before,
    gain_after,
    mixer_gain,
    layer_gain,
    layer_shift,
    spatial,
    spatial_shift,
    proj_gate,
    proj_lift,
    proj_down,
    mixer_u,
    mixer_v,
    mixer_down,
    out,
    gate_all,
    lift_all,
    down_all,
    u_all,
    v_all,
    mix_down_all,
    rows_all,
    to_sibling,
    from_sibling,
    to_chip,
    from_chip,
    part,
    hold,
    gate_vals,
    hidden,
    u_vals,
    lifted,
    gated,
    rows_last,
    hidden_last,
    part_half,
    masked,
    mom_own,
    mom_in,
    square,
    resid,
    local_sem,
    z_send,
    out_send,
    z_recv,
    y_send,
    y_recv,
    ag_sem,
    agf_sem,
    sib_sem,
    chip_sem,
    mom_sem,
    token_sem,
    second_sem,
):
    rep, fs, tp = lax.axis_index("rep"), lax.axis_index("fs"), lax.axis_index("tp")
    chip, core = tp // 2, lax.rem(tp, 2)
    n_chip = n_tp // 2
    block, width = stream.shape
    pair = 2 * block
    cols = width // n_fs
    shards = (proj_gate, proj_lift, proj_down, mixer_u, mixer_v, mixer_down)
    cuts = cuts_of(shards, n_rep)
    ahead, near_by = cuts + 2, cuts
    full = (gate_all, lift_all, down_all, u_all, v_all, mix_down_all)
    mine = pl.ds(pl.multiple_of(core * block, block), block)
    theirs = pl.ds(pl.multiple_of((1 - core) * block, block), block)
    sibling = chip * 2 + (1 - core)

    spread = n_fs >= 4
    depth = jnp.minimum(fs, n_fs - 1 - fs)
    side = (2 * fs) // n_fs
    inward = 1 - 2 * side
    if spread:
        low_slot = lax.rem(jnp.minimum(depth, 2) + 2, 3)
        at_end, at_mid = depth == 0, depth == 1
    else:
        low_slot = 1
    busy = low_slot < 2

    def when_busy(run):
        if spread:
            pl.when(busy)(run)
        else:
            run()

    def when_mid(run):
        if spread:
            pl.when(at_mid)(run)

    def when_end(run):
        if spread:
            pl.when(at_end)(run)

    def low_depth(w):
        return 1 if spread and w in MIXERS else 0

    def at(r, f, t):
        return (r, f, t)

    barrier = pltpu.get_barrier_semaphore()

    @pl.when(fs > 0)
    def _():
        pl.semaphore_signal(barrier, inc=1, device_id=at(rep, fs - 1, tp), device_id_type=MESH)

    @pl.when(fs < n_fs - 1)
    def _():
        pl.semaphore_signal(barrier, inc=1, device_id=at(rep, fs + 1, tp), device_id_type=MESH)

    for k in range(1, n_rep):
        pl.semaphore_signal(
            barrier, inc=1, device_id=at(lax.rem(rep + k, n_rep), fs, tp), device_id_type=MESH
        )
    for k in range(1, n_tp):
        pl.semaphore_signal(
            barrier, inc=1, device_id=at(rep, fs, lax.rem(tp + k, n_tp)), device_id_type=MESH
        )

    def depth_of(w):
        return shards[w].shape[0]

    def whole(w, owner):
        if w in BY_ROWS:
            n = depth_of(w)
            return full[w].at[pl.ds(pl.multiple_of(owner * n, n), n)]
        return full[w].at[owner]

    locals_ = [
        pltpu.make_async_copy(shards[w], whole(w, fs), local_sem.at[w]) for w in range(6)
    ]
    for copy in locals_:
        copy.start()

    line_peers = jnp.minimum(fs, 1) + jnp.minimum(n_fs - 1 - fs, 1)
    pl.semaphore_wait(barrier, n_rep - 1 + n_tp - 1 + line_peers)

    items = 6 * cuts

    def rows_of(w, owner, first_row, rows):
        if w in BY_ROWS:
            start = pl.multiple_of(owner * depth_of(w) + first_row, rows)
            return full[w].at[pl.ds(start, rows)]
        return full[w].at[owner, pl.ds(pl.multiple_of(first_row, rows), rows)]

    def piece(i, owner, part_index):
        w, cut = i // cuts, i % cuts
        rows = depth_of(w) // (n_rep * cuts)
        return rows_of(w, owner, (part_index * cuts + cut) * rows, rows)

    def share_of(w, owner, part_index):
        rows = depth_of(w) // n_rep
        return rows_of(w, owner, part_index * rows, rows)

    def settled(ref, send, recv):
        return pltpu.make_async_remote_copy(
            src_ref=ref, dst_ref=ref, send_sem=send, recv_sem=recv,
            device_id=at(lax.rem(rep + 1, n_rep), fs, tp), device_id_type=MESH,
        )

    def z_copy(i, owner, out, own_out=False):
        ref = piece(i, owner, rep)
        step = inward if out == 0 else -inward
        sem = out_send.at[i // cuts] if own_out else z_send.at[i // cuts, owner]
        return pltpu.make_async_remote_copy(
            src_ref=ref, dst_ref=ref, send_sem=sem,
            recv_sem=z_recv.at[i, owner],
            device_id=at(rep, fs + step, tp), device_id_type=MESH,
        )

    def rest_copy(i, k):
        ref = piece(i, fs, lax.rem(rep + n_rep - k, n_rep))
        return pltpu.make_async_remote_copy(
            src_ref=ref, dst_ref=ref, send_sem=y_send.at[i // cuts, k - 1, fs],
            recv_sem=y_recv.at[i // cuts, k - 1, fs],
            device_id=at(rep, fs + inward, tp), device_id_type=MESH,
        )

    def y_copy(i, owner, k):
        ref = piece(i, owner, rep)
        return pltpu.make_async_remote_copy(
            src_ref=ref, dst_ref=ref, send_sem=y_send.at[i // cuts, k - 1, owner],
            recv_sem=y_recv.at[i // cuts, k - 1, owner],
            device_id=at(lax.rem(rep + k, n_rep), fs, tp), device_id_type=MESH,
        )

    def own(i):
        w = i // cuts
        if i % cuts == 0:
            locals_[w].wait()
        if n_fs > 1:
            z_copy(i, fs, 0).start()

        @pl.when(depth > low_depth(w))
        def _():
            z_copy(i, fs, 1, True).start()

    def rest_end(i):
        for k in range(1, n_rep):
            rest_copy(i, k).start()

    def share(i, owner):
        for k in range(1, n_rep):
            y_copy(i, owner, k).start()

    def from_outer(i):
        w = i // cuts

        def hop(h, carry):
            @pl.when((depth >= h) & (depth >= low_depth(w)))
            def _():
                owner = fs - inward * h
                z_copy(i, owner, 0).wait_recv()
                z_copy(i, owner, 0).start()
                if spread:
                    pl.when((depth > 1) | (h > 1))(lambda: share(i, owner))
                else:
                    share(i, owner)

            return carry

        lax.fori_loop(1, (n_fs + 1) // 2, hop, 0)

    def from_inner(i, start, stop):
        w = i // cuts

        def hop(h, carry):
            @pl.when((depth + h < n_fs) & (depth >= low_depth(w)))
            def _():
                owner = fs + inward * h
                z_copy(i, owner, 1).wait_recv()

                @pl.when(depth > low_depth(w))
                def _():
                    z_copy(i, owner, 1).start()

                share(i, owner)

            return carry

        lax.fori_loop(start, stop, hop, 0)

    def near(i):
        if i < items and n_fs > 1:
            from_inner(i, 1, 2)

    def early(i):
        from_outer(i)
        if i < MIX_U * cuts - near_by:
            near(i + near_by)
        elif i >= MIX_U * cuts - 1:
            near(i + 1)

    def late(i):
        if n_fs > 2:
            from_inner(i, 2, n_fs)
        if i + ahead < items:
            when_busy(lambda: own(i + ahead))

    def y_share(w, owner, k, part_index):
        return settled(
            share_of(w, owner, part_index), y_send.at[w, k - 1, owner], y_recv.at[w, k - 1, owner]
        )

    def arrived_one(w, owner):
        for k in range(1, n_rep):
            y_share(w, owner, k, lax.rem(rep + n_rep - k, n_rep)).wait_recv()

    def arrived(w):
        def one(h, carry):
            arrived_one(w, lax.rem(fs + h, n_fs))
            return carry

        lax.fori_loop(1, n_fs, one, 0)

    def sends_done():
        def z_done(w, owner, send):
            settled(share_of(w, owner, rep), send, z_recv.at[w * cuts, owner]).wait_send()

        def one(owner, carry):
            offset = inward * (owner - fs)
            for w in range(6):
                low = low_depth(w)
                if n_fs > 1:
                    outer = (offset < 0) & (depth >= low)

                    @pl.when((offset == 0) | outer | ((offset > 0) & (depth > low)))
                    def _():
                        z_done(w, owner, z_send.at[w, owner])

                    @pl.when((offset == 0) & (depth > low))
                    def _():
                        z_done(w, owner, out_send.at[w])

                sent = (offset != 0) & (depth >= low)
                if spread:
                    sent = sent & ((depth != 1) | (offset != -1))

                @pl.when(sent)
                def _():
                    for k in range(1, n_rep):
                        y_share(w, owner, k, rep).wait_send()

            return carry

        lax.fori_loop(0, n_fs, one, 0)

        def rest():
            for w in range(6):
                for k in range(1, n_rep):
                    y_share(w, fs, k, lax.rem(rep + n_rep - k, n_rep)).wait_send()

        when_end(rest)

    def other_chip(k):
        return lax.rem(chip + k, n_chip)

    def source_chip(k):
        return lax.rem(chip + n_chip - k, n_chip)

    def tp_copy(src, dst, send, recv, target):
        return pltpu.make_async_remote_copy(
            src_ref=src, dst_ref=dst, send_sem=send, recv_sem=recv,
            device_id=at(rep, fs, target), device_id_type=MESH,
        )

    half = block // HALVES

    def gather_copy(phase, s, k, c):
        rows = pl.ds(pl.multiple_of(core * block + c * half, half), half)
        ref = rows_all.at[s, chip, rows]
        target = other_chip(k) * 2 + core
        return tp_copy(
            ref, ref, ag_sem.at[0, s, k - 1, c], ag_sem.at[1, s, k - 1, c], target
        )

    def pass_copy(phase, s, k):
        ref = rows_all.at[s, source_chip(k), mine]
        return tp_copy(ref, ref, agf_sem.at[0, s, k], agf_sem.at[1, s, k], sibling)

    def gather_send(phase, s, c):
        for k in range(1, n_chip):
            gather_copy(phase, s, k, c).start()

    def gather_start(phase, s, gain):
        rows_all[s, chip, mine] = norm_rows(resid[s].astype(jnp.float32), gain[...])
        gather_send(phase, s, 0)
        pass_copy(phase, s, 0).start()

    def gather_rest(phase, s):
        for c in range(1, HALVES):
            gather_send(phase, s, c)

    def gather_pass(phase, s):
        for k in range(1, n_chip):
            for c in range(HALVES):
                gather_copy(phase, s, k, c).wait_recv()
            pass_copy(phase, s, k).start()

    def gather_in(phase, s):
        for k in range(n_chip):
            pass_copy(phase, s, k).wait_recv()

    def gather_end(phase, s):
        for k in range(1, n_chip):
            for c in range(HALVES):
                gather_copy(phase, s, k, c).wait_send()
        for k in range(n_chip):
            pass_copy(phase, s, k).wait_send()

    def each_slot(run):
        def one(s, carry):
            run(s)
            return carry

        lax.fori_loop(low_slot, 2, one, 0)

    def each_pair(run):
        def one(p, carry):
            run(p)
            return carry

        lax.fori_loop(0, n_chip, one, 0)

    def sib_copy(s, p, f):
        return tp_copy(
            to_sibling.at[s, p, f], from_sibling.at[s, p, f],
            sib_sem.at[0, s, p, f], sib_sem.at[1, s, p, f], sibling,
        )

    def chip_copy(s, k, f):
        return tp_copy(
            to_chip.at[s, k - 1, f], from_chip.at[s, k - 1, f],
            chip_sem.at[0, s, k - 1, f], chip_sem.at[1, s, k - 1, f], other_chip(k) * 2 + core,
        )

    def product(s, p, f, left, w):
        part[...] = jnp.dot(left[s, p], full[w][f], preferred_element_type=jnp.float32)
        to_sibling[s, p, f] = part[theirs].astype(jnp.bfloat16)
        hold[s, p, f] = part[mine]
        sib_copy(s, p, f).start()

    def products(s, f, left, w):
        def one(k, carry):
            product(s, other_chip(k), f, left, w)
            return carry

        lax.fori_loop(1, n_chip + 1, one, 0)

    def joins(s, f):
        for k in range(1, n_chip):
            p = other_chip(k)
            sib_copy(s, p, f).wait_recv()
            joined = hold[s, p, f] + from_sibling[s, p, f].astype(jnp.float32)
            to_chip[s, k - 1, f] = joined.astype(jnp.bfloat16)
            chip_copy(s, k, f).start()

    def settle(s, f):
        sib_copy(s, chip, f).wait_recv()
        total = hold[s, chip, f] + from_sibling[s, chip, f].astype(jnp.float32)
        for k in range(1, n_chip):
            chip_copy(s, k, f).wait_recv()
            total = total + from_chip[s, k - 1, f].astype(jnp.float32)
        return total

    def reduce_end(s):
        def one(f, carry):
            for k in range(1, n_chip):
                chip_copy(s, k, f).wait_send()
            for p in range(n_chip):
                sib_copy(s, p, f).wait_send()
            return carry

        lax.fori_loop(0, n_fs, one, 0)

    def band(f):
        return pl.ds(pl.multiple_of(f * cols, cols), cols)

    def project(s, p, w):
        return jnp.dot(rows_all[s, p], full[w][...], preferred_element_type=jnp.float32)

    def gate_pair(s, p):
        gate_vals[s, p] = project(s, p, GATE)

    def lift_pair(s, p):
        hidden[s, p] = (jax.nn.silu(gate_vals[s, p]) * project(s, p, LIFT)).astype(jnp.bfloat16)

    def token_copy():
        return pltpu.make_async_remote_copy(
            src_ref=stream, dst_ref=resid.at[0], send_sem=token_sem.at[0],
            recv_sem=token_sem.at[1], device_id=at(rep, fs + inward, tp), device_id_type=MESH,
        )

    def second_copy(f):
        return pltpu.make_async_remote_copy(
            src_ref=resid.at[0, :, band(f)], dst_ref=resid.at[1, :, band(f)],
            send_sem=second_sem.at[0, f], recv_sem=second_sem.at[1, f],
            device_id=at(rep, fs - inward, tp), device_id_type=MESH,
        )

    def feed():
        token_copy().start()
        for w in range(6):
            for i in range(w * cuts, (w + 1) * cuts):
                own(i)
            for i in range(w * cuts, (w + 1) * cuts):
                rest_end(i)

    when_end(feed)

    def open_own():
        for i in range(ahead):
            own(i)
        resid[1] = stream[...]
        gather_start(0, 1, gain_before)
        gather_rest(0, 1)

    when_busy(open_own)
    for i in range(near_by):
        near(i)

    def open_guest():
        token_copy().wait_recv()
        gather_start(0, 0, gain_before)
        gather_rest(0, 0)

    def nth_owner(j):
        beyond = jnp.maximum(j - 1, 0)
        outs = jnp.minimum(beyond, depth)
        ins = beyond - outs
        first, far = jnp.minimum(beyond, 1), jnp.minimum(ins, 1)
        offset = (1 - first) * jnp.minimum(j, 1) + far * (ins + 1) - (first - far) * outs
        return fs + inward * offset

    when_mid(open_guest)

    def gates():
        each_slot(lambda s: gather_in(0, s))
        arrived(GATE)
        each_slot(lambda s: each_pair(lambda p: gate_pair(s, p)))

    def lifts(s):
        each_pair(lambda p: lift_pair(s, p))
        gather_end(0, s)

    def lifts_own():
        arrived(LIFT)
        lifts(1)
        products(1, fs, hidden, DOWN)
        joins(1, fs)

    def down_block(owner):
        each_slot(lambda s: products(s, owner, hidden, DOWN))
        each_slot(lambda s: joins(s, owner))

    def downs(start, stop):
        def one(j, carry):
            owner = nth_owner(j)
            arrived_one(DOWN, owner)
            down_block(owner)
            return carry

        lax.fori_loop(start, stop, one, 0)

    def first_band(s, j):
        f = nth_owner(j)
        base = resid[s, :, band(f)].astype(jnp.float32)
        resid[s, :, band(f)] = (base + 0.5 * settle(s, f)).astype(jnp.bfloat16)

    def first_bands(s, start, stop):
        def one(j, carry):
            first_band(s, j)
            return carry

        lax.fori_loop(start, stop, one, 0)

    def last_downs():
        downs(stops[2], stops[3])
        each_slot(lambda s: first_bands(s, 0, n_fs - 1))

    def first_of(s):
        first_bands(s, n_fs - 1, n_fs)
        gather_start(1, s, mixer_gain)

    def guest_first():
        first_of(0)
        gather_rest(1, 0)

    def own_first():
        first_of(1)
        gather_rest(1, 1)
        each_slot(reduce_end)

    def guest_lifts():
        lifts(0)
        products(0, fs, hidden, DOWN)
        joins(0, fs)

    stops = [1 + (n_fs - 1) * t // 3 for t in range(4)]

    def far_downs():
        downs(stops[2], stops[3])
        each_slot(lambda s: first_bands(s, 0, n_fs - 1))

    groups = spatial.shape[0]
    channels = lifted.shape[3]
    group_dim = channels // groups
    all_channels = channels * n_tp

    def u_pair(s, p):
        u_vals[s, p] = jax.nn.gelu(project(s, p, MIX_U))

    def v_pair(s, p):
        values = jax.nn.gelu(project(s, p, MIX_V))
        lifted[s, p] = values
        sums = jnp.sum(values, axis=1, keepdims=True)
        squares = jnp.sum(values * values, axis=1, keepdims=True)
        lane = lax.broadcasted_iota(jnp.int32, (pair, 128), 1)
        both = jnp.where(lane == 0, sums, jnp.where(lane == 1, squares, 0.0))
        mom_own[s, p] = both.T[:8]

    def mom_copy(s, k):
        return tp_copy(
            mom_own.at[s], mom_in.at[s, k - 1], mom_sem.at[0, s, k - 1], mom_sem.at[1, s, k - 1],
            lax.rem(tp + k, n_tp),
        )

    def values_of(s):
        gather_pass(1, s)
        gather_in(1, s)
        each_pair(lambda p: v_pair(s, p))
        for k in range(1, n_tp):
            mom_copy(s, k).start()
        each_pair(lambda p: u_pair(s, p))
        gather_end(1, s)

    def mix_of(s):
        for k in range(1, n_tp):
            mom_copy(s, k).wait_recv()
        shift_columns = square[...].T

        def mix_pair(p):
            moments = mom_own[s, p]
            for k in range(1, n_tp):
                moments = moments + mom_in[s, k - 1, p]
            moments = moments * (1.0 / all_channels)
            columns = jnp.concatenate([moments, jnp.zeros((120, pair), jnp.float32)], axis=0).T
            centre = columns[:, 0:1]
            spread_of = columns[:, 1:2] - centre * centre
            normed_v = (
                (lifted[s, p] - centre) * lax.rsqrt(spread_of + layer_epsilon) * layer_gain[...]
                + layer_shift[...]
            ).astype(jnp.bfloat16)
            for g in range(groups):
                cut = slice(g * group_dim, (g + 1) * group_dim)
                for b in range(pair // SPAN):
                    span = slice(b * SPAN, (b + 1) * SPAN)
                    mixed = jnp.dot(
                        masked[g], normed_v[span, cut], preferred_element_type=jnp.float32
                    )
                    mixed = mixed + shift_columns[:, g : g + 1]
                    gated[s, p, span, cut] = (u_vals[s, p, span, cut] * mixed).astype(jnp.bfloat16)

        each_pair(mix_pair)
        for k in range(1, n_tp):
            mom_copy(s, k).wait_send()

    def guest_values():
        values_of(0)

    def mixer_in():
        row = lax.broadcasted_iota(jnp.int32, (SPAN, SPAN), 0)
        col = lax.broadcasted_iota(jnp.int32, (SPAN, SPAN), 1)
        for g in range(groups):
            masked[g] = jnp.where(row >= col, spatial[g].astype(jnp.float32), 0.0).astype(
                jnp.bfloat16
            )
        square[...] = jnp.zeros_like(square)
        square[0:groups, :] = spatial_shift[...]
        arrived(MIX_U)
        arrived(MIX_V)
        when_mid(guest_values)


    between = {
        (GATE, 0): lambda: when_busy(lambda: gather_pass(0, 1)),
        (GATE, 3): lambda: when_mid(lambda: gather_pass(0, 0)),
        (LIFT, 2): lambda: when_busy(gates),
        (DOWN, 0): lambda: when_busy(lifts_own),
        (DOWN, 1): lambda: when_mid(guest_lifts),
        (DOWN, 2): lambda: when_busy(lambda: downs(stops[0], stops[1])),
        (DOWN, 3): lambda: when_busy(lambda: downs(stops[1], stops[2])),
        (MIX_U, 1): lambda: when_busy(far_downs),
        (MIX_U, 3): lambda: when_mid(guest_first),
        (MIX_V, 1): lambda: when_busy(own_first),
        (MIX_DOWN, 1): lambda: when_busy(mixer_in),
    }
    for w in range(6):
        for stage, step in enumerate((early, late)):
            for i in range(w * cuts, (w + 1) * cuts):
                step(i)
                for place, edge in enumerate((w * cuts, (w + 1) * cuts - 1)):
                    if i == edge and (w, 2 * stage + place) in between:
                        between[w, 2 * stage + place]()

    def bands_of(start, stop, run):
        def one(h, carry):
            run(nth_owner(h))
            return carry

        lax.fori_loop(start, stop, one, 0)

    def span_of(s, start, stop):
        bands_of(start, stop, lambda f: products(s, f, gated, MIX_DOWN))
        bands_of(start, stop, lambda f: joins(s, f))

    def second_band(s, f):
        base = resid[s, :, band(f)].astype(jnp.float32)
        resid[s, :, band(f)] = (base + settle(s, f)).astype(jnp.bfloat16)

    def ship(start, stop):
        def one(f):
            second_band(0, f)
            second_copy(f).start()

        bands_of(start, stop, one)

    def mixer_out():
        middle = n_fs // 2

        def guest_in():
            mix_of(0)
            bands_of(1, middle, lambda f: arrived_one(MIX_DOWN, f))
            span_of(0, 0, middle)

        def guest_rest():
            bands_of(middle, n_fs, lambda f: arrived_one(MIX_DOWN, f))
            span_of(0, middle, n_fs)
            ship(0, middle)

        def guest_ship():
            ship(middle, n_fs)
            reduce_end(0)

        when_mid(guest_in)
        values_of(1)
        if spread:
            pl.when(depth > 1)(lambda: arrived(MIX_DOWN))
        else:
            arrived(MIX_DOWN)
        when_mid(guest_rest)
        mix_of(1)
        span_of(1, 0, n_fs)
        when_mid(guest_ship)
        bands_of(0, n_fs, lambda f: second_band(1, f))
        reduce_end(1)

    when_busy(mixer_out)

    def close_guest():
        arrived(GATE)
        arrived(LIFT)
        arrived(DOWN)
        for f in range(n_fs):
            second_copy(f).wait_recv()

    when_end(close_guest)
    def gather_half(k, c):
        ref = rows_last.at[chip, c, core]
        target = other_chip(k) * 2 + core
        return tp_copy(ref, ref, ag_sem.at[0, 1, k - 1, c], ag_sem.at[1, 1, k - 1, c], target)

    def pass_half(k, c):
        ref = rows_last.at[source_chip(k), c, core]
        return tp_copy(ref, ref, agf_sem.at[0, c, k], agf_sem.at[1, c, k], sibling)

    def sib_half(p, f, c):
        rows = pl.ds(c * half, half)
        return tp_copy(
            to_sibling.at[1, p, f, rows], from_sibling.at[1, p, f, rows],
            sib_sem.at[0, c, p, f], sib_sem.at[1, c, p, f], sibling,
        )

    def chip_half(k, f, c):
        rows = pl.ds(c * half, half)
        return tp_copy(
            to_chip.at[1, k - 1, f, rows], from_chip.at[1, k - 1, f, rows],
            chip_sem.at[0, c, k - 1, f], chip_sem.at[1, c, k - 1, f], other_chip(k) * 2 + core,
        )

    normed = norm_rows(resid[1].astype(jnp.float32), gain_after[...])
    for c in range(HALVES):
        rows_last[chip, c, core] = normed[c * half : (c + 1) * half]
        for k in range(1, n_chip):
            gather_half(k, c).start()
        pass_half(0, c).start()

    def last_rows(p, c):
        rows = rows_last[p, c].reshape(2 * half, width)
        gate = jnp.dot(rows, full[GATE][...], preferred_element_type=jnp.float32)
        lift = jnp.dot(rows, full[LIFT][...], preferred_element_type=jnp.float32)
        hidden_last[p, c] = (jax.nn.silu(gate) * lift).astype(jnp.bfloat16)

    def last_products(p, c):
        def one(f, carry):
            part_half[...] = jnp.dot(
                hidden_last[p, c], full[DOWN][f], preferred_element_type=jnp.float32
            ).reshape(part_half.shape)
            rows = pl.ds(c * half, half)
            to_sibling[1, p, f, rows] = part_half[1 - core].astype(jnp.bfloat16)
            hold[1, p, f, rows] = part_half[core]
            sib_half(p, f, c).start()
            return carry

        lax.fori_loop(0, n_fs, one, 0)

    def last_joins(k, c):
        p = other_chip(k)

        def one(f, carry):
            rows = pl.ds(c * half, half)
            sib_half(p, f, c).wait_recv()
            joined = hold[1, p, f, rows] + from_sibling[1, p, f, rows].astype(jnp.float32)
            to_chip[1, k - 1, f, rows] = joined.astype(jnp.bfloat16)
            chip_half(k, f, c).start()
            return carry

        lax.fori_loop(0, n_fs, one, 0)

    for c in range(HALVES):
        pass_half(0, c).wait_recv()
        last_rows(chip, c)

    when_end(lambda: token_copy().wait_send())

    def shipped():
        for f in range(n_fs):
            second_copy(f).wait_send()

    when_mid(shipped)
    sends_done()

    for c in range(HALVES):
        for k in range(1, n_chip):
            gather_half(k, c).wait_recv()
            pass_half(k, c).start()
        for k in range(1, n_chip):
            pass_half(k, c).wait_recv()
            last_rows(other_chip(k), c)
            last_products(other_chip(k), c)
        for k in range(1, n_chip):
            last_joins(k, c)
        last_products(chip, c)
    for f in range(n_fs):
        for c in range(HALVES):
            sib_half(chip, f, c).wait_recv()
        total = hold[1, chip, f] + from_sibling[1, chip, f].astype(jnp.float32)
        for k in range(1, n_chip):
            for c in range(HALVES):
                chip_half(k, f, c).wait_recv()
            total = total + from_chip[1, k - 1, f].astype(jnp.float32)
        base = resid[1, :, band(f)].astype(jnp.float32)
        out[:, band(f)] = (base + 0.5 * total).astype(jnp.bfloat16)
    for c in range(HALVES):
        for k in range(n_chip):
            pass_half(k, c).wait_send()
        for k in range(1, n_chip):
            gather_half(k, c).wait_send()

    def last_sent(f, carry):
        for c in range(HALVES):
            for p in range(n_chip):
                sib_half(p, f, c).wait_send()
            for k in range(1, n_chip):
                chip_half(k, f, c).wait_send()
        return carry

    lax.fori_loop(0, n_fs, last_sent, 0)


def body(
    n_rep,
    n_fs,
    n_tp,
    stream,
    gain_before,
    gain_after,
    proj_gate,
    proj_lift,
    proj_down,
    mixer_gain,
    mixer_u,
    mixer_v,
    layer_gain,
    layer_shift,
    spatial,
    spatial_shift,
    mixer_down,
):
    block, width = stream.shape
    n_chip = n_tp // 2
    pair = 2 * block
    cols = width // n_fs
    units = proj_gate.shape[1]
    channels = mixer_u.shape[1]
    bf16, f32 = jnp.bfloat16, jnp.float32
    shards = (proj_gate, proj_lift, proj_down, mixer_u, mixer_v, mixer_down)
    cuts = cuts_of(shards, n_rep)
    vmem = pl.BlockSpec(memory_space=pltpu.VMEM)
    anywhere = pl.BlockSpec(memory_space=pl.ANY)
    dma = pltpu.SemaphoreType.DMA
    spread_reps = max(n_rep - 1, 1)
    spread_chips = max(n_chip - 1, 1)
    return pl.pallas_call(
        functools.partial(layer_kernel, n_rep, n_fs, n_tp),
        out_shape=pltpu.VMEM((block, width), bf16),
        in_specs=[vmem] * 8 + [anywhere] * 6,
        out_specs=vmem,
        scratch_shapes=[
            pltpu.VMEM(
                (n_fs * w.shape[0], w.shape[1]) if i in BY_ROWS else (n_fs,) + w.shape, bf16
            )
            for i, w in enumerate(shards)
        ]
        + [
            pltpu.VMEM((2, n_chip, pair, width), bf16),
            pltpu.VMEM((2, n_chip, n_fs, block, cols), bf16),
            pltpu.VMEM((2, n_chip, n_fs, block, cols), bf16),
            pltpu.VMEM((2, spread_chips, n_fs, block, cols), bf16),
            pltpu.VMEM((2, spread_chips, n_fs, block, cols), bf16),
            pltpu.VMEM((pair, cols), f32),
            pltpu.VMEM((2, n_chip, n_fs, block, cols), f32),
            pltpu.VMEM((2, n_chip, pair, units), f32),
            pltpu.VMEM((2, n_chip, pair, units), bf16),
            pltpu.VMEM((2, n_chip, pair, channels), f32),
            pltpu.VMEM((2, n_chip, pair, channels), f32),
            pltpu.VMEM((2, n_chip, pair, channels), bf16),
            pltpu.VMEM((n_chip, HALVES, 2, block // HALVES, width), bf16),
            pltpu.VMEM((n_chip, HALVES, 2 * block // HALVES, units), bf16),
            pltpu.VMEM((2, block // HALVES, cols), f32),
            pltpu.VMEM(spatial.shape, bf16),
            pltpu.VMEM((2, n_chip, 8, pair), f32),
            pltpu.VMEM((2, max(n_tp - 1, 1), n_chip, 8, pair), f32),
            pltpu.VMEM((128, SPAN), f32),
            pltpu.VMEM((2, block, width), bf16),
            dma((6,)),
            dma((6, n_fs)),
            dma((6,)),
            dma((6 * cuts, n_fs)),
            dma((6, spread_reps, n_fs)),
            dma((6, spread_reps, n_fs)),
            dma((2, 2, spread_chips, HALVES)),
            dma((2, 2, n_chip)),
            dma((2, 2, n_chip, n_fs)),
            dma((2, 2, spread_chips, n_fs)),
            dma((2, 2, max(n_tp - 1, 1))),
            dma((2,)),
            dma((2, n_fs)),
        ],
        compiler_params=pltpu.CompilerParams(
            collective_id=0, has_side_effects=True, vmem_limit_bytes=60 * 1024 * 1024
        ),
    )(
        stream,
        gain_before.reshape(1, -1),
        gain_after.reshape(1, -1),
        mixer_gain.reshape(1, -1),
        layer_gain.reshape(1, -1),
        layer_shift.reshape(1, -1),
        spatial,
        spatial_shift,
        *shards,
    )


def solution(mesh):
    placed = (
        P(("rep", "fs", "tp"), None),
        P(),
        P(),
        P("fs", "tp"),
        P("fs", "tp"),
        P("tp", "fs"),
        P(),
        P("fs", "tp"),
        P("fs", "tp"),
        P("tp"),
        P("tp"),
        P("tp", None, None),
        P("tp", None),
        P("tp", "fs"),
    )
    sizes = (mesh.shape["rep"], mesh.shape["fs"], mesh.shape["tp"])
    return jax.shard_map(
        functools.partial(body, *sizes),
        mesh=mesh,
        in_specs=placed,
        out_specs=P(("rep", "fs", "tp"), None),
        check_vma=False,
    )
```

```python
import functools

import jax
import jax.numpy as jnp
from jax import lax
from jax.experimental import pallas as pl
from jax.experimental.pallas import tpu as pltpu
from jax.sharding import PartitionSpec as P

SPAN = 128

norm_epsilon = 1e-06
layer_epsilon = 1e-05

MESH = pl.DeviceIdType.MESH
GATE, LIFT, DOWN, MIX_U, MIX_V, MIX_DOWN = range(6)
HALVES = 2
MIXERS = (MIX_U, MIX_V, MIX_DOWN)
BY_ROWS = (GATE, LIFT, MIX_U, MIX_V)


def cuts_of(shards, n_rep):
    return 2 if all(w.shape[0] % (n_rep * 32) == 0 for w in shards) else 1


def norm_rows(widened, scale_gain):
    factor = lax.rsqrt(jnp.mean(widened * widened, axis=1, keepdims=True) + norm_epsilon)
    return (widened * factor * scale_gain).astype(jnp.bfloat16)


def layer_kernel(
    n_rep,
    n_fs,
    n_tp,
    stream,
    gain_before,
    gain_after,
    mixer_gain,
    layer_gain,
    layer_shift,
    spatial,
    spatial_shift,
    proj_gate,
    proj_lift,
    proj_down,
    mixer_u,
    mixer_v,
    mixer_down,
    out,
    gate_all,
    lift_all,
    down_all,
    u_all,
    v_all,
    mix_down_all,
    rows_all,
    to_sibling,
    from_sibling,
    to_chip,
    from_chip,
    part,
    hold,
    gate_vals,
    hidden,
    u_vals,
    lifted,
    gated,
    rows_last,
    hidden_last,
    part_half,
    masked,
    mom_own,
    mom_in,
    square,
    resid,
    local_sem,
    z_send,
    out_send,
    z_recv,
    y_send,
    y_recv,
    ag_sem,
    agf_sem,
    sib_sem,
    chip_sem,
    mom_sem,
    token_sem,
    second_sem,
):
    rep, fs, tp = lax.axis_index("rep"), lax.axis_index("fs"), lax.axis_index("tp")
    chip, core = tp // 2, lax.rem(tp, 2)
    n_chip = n_tp // 2
    block, width = stream.shape
    pair = 2 * block
    cols = width // n_fs
    shards = (proj_gate, proj_lift, proj_down, mixer_u, mixer_v, mixer_down)
    cuts = cuts_of(shards, n_rep)
    ahead, near_by = cuts + 2, cuts
    full = (gate_all, lift_all, down_all, u_all, v_all, mix_down_all)
    mine = pl.ds(pl.multiple_of(core * block, block), block)
    theirs = pl.ds(pl.multiple_of((1 - core) * block, block), block)
    sibling = chip * 2 + (1 - core)

    spread = n_fs >= 4
    depth = jnp.minimum(fs, n_fs - 1 - fs)
    side = (2 * fs) // n_fs
    inward = 1 - 2 * side
    if spread:
        low_slot = lax.rem(jnp.minimum(depth, 2) + 2, 3)
        at_end, at_mid = depth == 0, depth == 1
    else:
        low_slot = 1
    busy = low_slot < 2

    def when_busy(run):
        if spread:
            pl.when(busy)(run)
        else:
            run()

    def when_mid(run):
        if spread:
            pl.when(at_mid)(run)

    def when_end(run):
        if spread:
            pl.when(at_end)(run)

    def low_depth(w):
        return 1 if spread and w in MIXERS else 0

    def at(r, f, t):
        return (r, f, t)

    barrier = pltpu.get_barrier_semaphore()

    @pl.when(fs > 0)
    def _():
        pl.semaphore_signal(barrier, inc=1, device_id=at(rep, fs - 1, tp), device_id_type=MESH)

    @pl.when(fs < n_fs - 1)
    def _():
        pl.semaphore_signal(barrier, inc=1, device_id=at(rep, fs + 1, tp), device_id_type=MESH)

    for k in range(1, n_rep):
        pl.semaphore_signal(
            barrier, inc=1, device_id=at(lax.rem(rep + k, n_rep), fs, tp), device_id_type=MESH
        )
    for k in range(1, n_tp):
        pl.semaphore_signal(
            barrier, inc=1, device_id=at(rep, fs, lax.rem(tp + k, n_tp)), device_id_type=MESH
        )

    def depth_of(w):
        return shards[w].shape[0]

    def whole(w, owner):
        if w in BY_ROWS:
            n = depth_of(w)
            return full[w].at[pl.ds(pl.multiple_of(owner * n, n), n)]
        return full[w].at[owner]

    locals_ = [
        pltpu.make_async_copy(shards[w], whole(w, fs), local_sem.at[w]) for w in range(6)
    ]
    first_slot = jnp.minimum(depth, 1) if spread else 1
    stream_in = pltpu.make_async_copy(stream, resid.at[first_slot], local_sem.at[6])
    spatial_in = pltpu.make_async_copy(spatial, masked, local_sem.at[7])
    for copy in [stream_in] + locals_ + [spatial_in]:
        copy.start()

    line_peers = jnp.minimum(fs, 1) + jnp.minimum(n_fs - 1 - fs, 1)
    pl.semaphore_wait(barrier, n_rep - 1 + n_tp - 1 + line_peers)
    stream_in.wait()

    items = 6 * cuts

    def rows_of(w, owner, first_row, rows):
        if w in BY_ROWS:
            start = pl.multiple_of(owner * depth_of(w) + first_row, rows)
            return full[w].at[pl.ds(start, rows)]
        return full[w].at[owner, pl.ds(pl.multiple_of(first_row, rows), rows)]

    def piece(i, owner, part_index):
        w, cut = i // cuts, i % cuts
        rows = depth_of(w) // (n_rep * cuts)
        return rows_of(w, owner, (part_index * cuts + cut) * rows, rows)

    def share_of(w, owner, part_index):
        rows = depth_of(w) // n_rep
        return rows_of(w, owner, part_index * rows, rows)

    def settled(ref, send, recv):
        return pltpu.make_async_remote_copy(
            src_ref=ref, dst_ref=ref, send_sem=send, recv_sem=recv,
            device_id=at(lax.rem(rep + 1, n_rep), fs, tp), device_id_type=MESH,
        )

    def z_copy(i, owner, out, own_out=False):
        ref = piece(i, owner, rep)
        step = inward if out == 0 else -inward
        sem = out_send.at[i // cuts] if own_out else z_send.at[i // cuts, owner]
        return pltpu.make_async_remote_copy(
            src_ref=ref, dst_ref=ref, send_sem=sem,
            recv_sem=z_recv.at[i, owner],
            device_id=at(rep, fs + step, tp), device_id_type=MESH,
        )

    def rest_copy(i, k):
        ref = piece(i, fs, lax.rem(rep + n_rep - k, n_rep))
        return pltpu.make_async_remote_copy(
            src_ref=ref, dst_ref=ref, send_sem=y_send.at[i // cuts, k - 1, fs],
            recv_sem=y_recv.at[i // cuts, k - 1, fs],
            device_id=at(rep, fs + inward, tp), device_id_type=MESH,
        )

    def y_copy(i, owner, k):
        ref = piece(i, owner, rep)
        return pltpu.make_async_remote_copy(
            src_ref=ref, dst_ref=ref, send_sem=y_send.at[i // cuts, k - 1, owner],
            recv_sem=y_recv.at[i // cuts, k - 1, owner],
            device_id=at(lax.rem(rep + k, n_rep), fs, tp), device_id_type=MESH,
        )

    def own(i):
        w = i // cuts
        if i % cuts == 0:
            locals_[w].wait()
        if n_fs > 1:
            z_copy(i, fs, 0).start()

        @pl.when(depth > low_depth(w))
        def _():
            z_copy(i, fs, 1, True).start()

    def rest_end(i):
        for k in range(1, n_rep):
            rest_copy(i, k).start()

    def share(i, owner):
        for k in range(1, n_rep):
            y_copy(i, owner, k).start()

    def from_outer(i):
        w = i // cuts

        def hop(h, carry):
            @pl.when((depth >= h) & (depth >= low_depth(w)))
            def _():
                owner = fs - inward * h
                z_copy(i, owner, 0).wait_recv()
                z_copy(i, owner, 0).start()
                if spread:
                    pl.when((depth > 1) | (h > 1))(lambda: share(i, owner))
                else:
                    share(i, owner)

            return carry

        lax.fori_loop(1, (n_fs + 1) // 2, hop, 0)

    def from_inner(i, start, stop):
        w = i // cuts

        def hop(h, carry):
            @pl.when((depth + h < n_fs) & (depth >= low_depth(w)))
            def _():
                owner = fs + inward * h
                z_copy(i, owner, 1).wait_recv()

                @pl.when(depth > low_depth(w))
                def _():
                    z_copy(i, owner, 1).start()

                share(i, owner)

            return carry

        lax.fori_loop(start, stop, hop, 0)

    def near(i):
        if i < items and n_fs > 1:
            from_inner(i, 1, 2)

    def early(i):
        from_outer(i)
        if i < MIX_U * cuts - near_by:
            near(i + near_by)
        elif i >= MIX_U * cuts - 1:
            near(i + 1)

    def late(i):
        if n_fs > 2:
            from_inner(i, 2, n_fs)
        if i + ahead < items:
            when_busy(lambda: own(i + ahead))

    def y_share(w, owner, k, part_index):
        return settled(
            share_of(w, owner, part_index), y_send.at[w, k - 1, owner], y_recv.at[w, k - 1, owner]
        )

    def arrived_one(w, owner):
        for k in range(1, n_rep):
            y_share(w, owner, k, lax.rem(rep + n_rep - k, n_rep)).wait_recv()

    def arrived(w):
        def one(h, carry):
            arrived_one(w, lax.rem(fs + h, n_fs))
            return carry

        lax.fori_loop(1, n_fs, one, 0)

    def sends_done():
        def z_done(w, owner, send):
            settled(share_of(w, owner, rep), send, z_recv.at[w * cuts, owner]).wait_send()

        def one(owner, carry):
            offset = inward * (owner - fs)
            for w in range(6):
                low = low_depth(w)
                if n_fs > 1:
                    outer = (offset < 0) & (depth >= low)

                    @pl.when((offset == 0) | outer | ((offset > 0) & (depth > low)))
                    def _():
                        z_done(w, owner, z_send.at[w, owner])

                    @pl.when((offset == 0) & (depth > low))
                    def _():
                        z_done(w, owner, out_send.at[w])

                sent = (offset != 0) & (depth >= low)
                if spread:
                    sent = sent & ((depth != 1) | (offset != -1))

                @pl.when(sent)
                def _():
                    for k in range(1, n_rep):
                        y_share(w, owner, k, rep).wait_send()

            return carry

        lax.fori_loop(0, n_fs, one, 0)

        def rest():
            for w in range(6):
                for k in range(1, n_rep):
                    y_share(w, fs, k, lax.rem(rep + n_rep - k, n_rep)).wait_send()

        when_end(rest)

    def other_chip(k):
        return lax.rem(chip + k, n_chip)

    def source_chip(k):
        return lax.rem(chip + n_chip - k, n_chip)

    def tp_copy(src, dst, send, recv, target):
        return pltpu.make_async_remote_copy(
            src_ref=src, dst_ref=dst, send_sem=send, recv_sem=recv,
            device_id=at(rep, fs, target), device_id_type=MESH,
        )

    half = block // HALVES

    def gather_copy(phase, s, k, c):
        rows = pl.ds(pl.multiple_of(core * block + c * half, half), half)
        ref = rows_all.at[s, chip, rows]
        target = other_chip(k) * 2 + core
        return tp_copy(
            ref, ref, ag_sem.at[0, s, k - 1, c], ag_sem.at[1, s, k - 1, c], target
        )

    def pass_copy(phase, s, k):
        ref = rows_all.at[s, source_chip(k), mine]
        return tp_copy(ref, ref, agf_sem.at[0, s, k], agf_sem.at[1, s, k], sibling)

    def gather_send(phase, s, c):
        for k in range(1, n_chip):
            gather_copy(phase, s, k, c).start()

    def gather_start(phase, s, gain):
        rows_all[s, chip, mine] = norm_rows(resid[s].astype(jnp.float32), gain[...])
        gather_send(phase, s, 0)
        pass_copy(phase, s, 0).start()

    def gather_rest(phase, s):
        for c in range(1, HALVES):
            gather_send(phase, s, c)

    def gather_pass(phase, s):
        for k in range(1, n_chip):
            for c in range(HALVES):
                gather_copy(phase, s, k, c).wait_recv()
            pass_copy(phase, s, k).start()

    def gather_in(phase, s):
        for k in range(n_chip):
            pass_copy(phase, s, k).wait_recv()

    def gather_end(phase, s):
        for k in range(1, n_chip):
            for c in range(HALVES):
                gather_copy(phase, s, k, c).wait_send()
        for k in range(n_chip):
            pass_copy(phase, s, k).wait_send()

    def each_slot(run):
        def one(s, carry):
            run(s)
            return carry

        lax.fori_loop(low_slot, 2, one, 0)

    def each_pair(run):
        def one(p, carry):
            run(p)
            return carry

        lax.fori_loop(0, n_chip, one, 0)

    def sib_copy(s, p, f):
        return tp_copy(
            to_sibling.at[s, p, f], from_sibling.at[s, p, f],
            sib_sem.at[0, s, p, f], sib_sem.at[1, s, p, f], sibling,
        )

    def chip_copy(s, k, f):
        return tp_copy(
            to_chip.at[s, k - 1, f], from_chip.at[s, k - 1, f],
            chip_sem.at[0, s, k - 1, f], chip_sem.at[1, s, k - 1, f], other_chip(k) * 2 + core,
        )

    def product(s, p, f, left, w):
        part[...] = jnp.dot(left[s, p], full[w][f], preferred_element_type=jnp.float32)
        to_sibling[s, p, f] = part[theirs].astype(jnp.bfloat16)
        hold[s, p, f] = part[mine]
        sib_copy(s, p, f).start()

    def products(s, f, left, w):
        def one(k, carry):
            product(s, other_chip(k), f, left, w)
            return carry

        lax.fori_loop(1, n_chip + 1, one, 0)

    def joins(s, f):
        for k in range(1, n_chip):
            p = other_chip(k)
            sib_copy(s, p, f).wait_recv()
            joined = hold[s, p, f] + from_sibling[s, p, f].astype(jnp.float32)
            to_chip[s, k - 1, f] = joined.astype(jnp.bfloat16)
            chip_copy(s, k, f).start()

    def settle(s, f):
        sib_copy(s, chip, f).wait_recv()
        total = hold[s, chip, f] + from_sibling[s, chip, f].astype(jnp.float32)
        for k in range(1, n_chip):
            chip_copy(s, k, f).wait_recv()
            total = total + from_chip[s, k - 1, f].astype(jnp.float32)
        return total

    def reduce_end(s):
        def one(f, carry):
            for k in range(1, n_chip):
                chip_copy(s, k, f).wait_send()
            for p in range(n_chip):
                sib_copy(s, p, f).wait_send()
            return carry

        lax.fori_loop(0, n_fs, one, 0)

    def band(f):
        return pl.ds(pl.multiple_of(f * cols, cols), cols)

    def project(s, p, w):
        return jnp.dot(rows_all[s, p], full[w][...], preferred_element_type=jnp.float32)

    def gate_pair(s, p):
        gate_vals[s, p] = project(s, p, GATE)

    def lift_pair(s, p):
        hidden[s, p] = (jax.nn.silu(gate_vals[s, p]) * project(s, p, LIFT)).astype(jnp.bfloat16)

    def token_copy():
        return pltpu.make_async_remote_copy(
            src_ref=resid.at[0], dst_ref=resid.at[0], send_sem=token_sem.at[0],
            recv_sem=token_sem.at[1], device_id=at(rep, fs + inward, tp), device_id_type=MESH,
        )

    def second_copy(f):
        return pltpu.make_async_remote_copy(
            src_ref=resid.at[0, :, band(f)], dst_ref=resid.at[1, :, band(f)],
            send_sem=second_sem.at[0, f], recv_sem=second_sem.at[1, f],
            device_id=at(rep, fs - inward, tp), device_id_type=MESH,
        )

    def feed():
        token_copy().start()
        for w in range(6):
            for i in range(w * cuts, (w + 1) * cuts):
                own(i)
            for i in range(w * cuts, (w + 1) * cuts):
                rest_end(i)

    when_end(feed)

    def open_own():
        for i in range(ahead):
            own(i)
        gather_start(0, 1, gain_before)
        gather_rest(0, 1)

    when_busy(open_own)
    spatial_in.wait()
    for i in range(near_by):
        near(i)

    def open_guest():
        token_copy().wait_recv()
        gather_start(0, 0, gain_before)
        gather_rest(0, 0)

    def nth_owner(j):
        beyond = jnp.maximum(j - 1, 0)
        outs = jnp.minimum(beyond, depth)
        ins = beyond - outs
        first, far = jnp.minimum(beyond, 1), jnp.minimum(ins, 1)
        offset = (1 - first) * jnp.minimum(j, 1) + far * (ins + 1) - (first - far) * outs
        return fs + inward * offset

    when_mid(open_guest)

    def gates():
        each_slot(lambda s: gather_in(0, s))
        arrived(GATE)
        each_slot(lambda s: each_pair(lambda p: gate_pair(s, p)))

    def lifts(s):
        each_pair(lambda p: lift_pair(s, p))
        gather_end(0, s)

    def lifts_own():
        arrived(LIFT)
        lifts(1)
        products(1, fs, hidden, DOWN)
        joins(1, fs)

    def down_block(owner):
        each_slot(lambda s: products(s, owner, hidden, DOWN))
        each_slot(lambda s: joins(s, owner))

    def downs(start, stop):
        def one(j, carry):
            owner = nth_owner(j)
            arrived_one(DOWN, owner)
            down_block(owner)
            return carry

        lax.fori_loop(start, stop, one, 0)

    def first_band(s, j):
        f = nth_owner(j)
        base = resid[s, :, band(f)].astype(jnp.float32)
        resid[s, :, band(f)] = (base + 0.5 * settle(s, f)).astype(jnp.bfloat16)

    def first_bands(s, start, stop):
        def one(j, carry):
            first_band(s, j)
            return carry

        lax.fori_loop(start, stop, one, 0)

    def last_downs():
        downs(stops[2], stops[3])
        each_slot(lambda s: first_bands(s, 0, n_fs - 1))

    def first_of(s):
        first_bands(s, n_fs - 1, n_fs)
        gather_start(1, s, mixer_gain)

    def guest_first():
        first_of(0)
        gather_rest(1, 0)

    def own_first():
        first_of(1)
        gather_rest(1, 1)
        each_slot(reduce_end)

    def guest_lifts():
        lifts(0)
        products(0, fs, hidden, DOWN)
        joins(0, fs)

    stops = [1 + (n_fs - 1) * t // 3 for t in range(4)]

    def far_downs():
        downs(stops[2], stops[3])
        each_slot(lambda s: first_bands(s, 0, n_fs - 1))

    groups = spatial.shape[0]
    channels = lifted.shape[3]
    group_dim = channels // groups
    all_channels = channels * n_tp

    def u_pair(s, p):
        u_vals[s, p] = jax.nn.gelu(project(s, p, MIX_U))

    def v_pair(s, p):
        values = jax.nn.gelu(project(s, p, MIX_V))
        lifted[s, p] = values
        sums = jnp.sum(values, axis=1, keepdims=True)
        squares = jnp.sum(values * values, axis=1, keepdims=True)
        lane = lax.broadcasted_iota(jnp.int32, (pair, 128), 1)
        both = jnp.where(lane == 0, sums, jnp.where(lane == 1, squares, 0.0))
        mom_own[s, p] = both.T[:8]

    def mom_copy(s, k):
        return tp_copy(
            mom_own.at[s], mom_in.at[s, k - 1], mom_sem.at[0, s, k - 1], mom_sem.at[1, s, k - 1],
            lax.rem(tp + k, n_tp),
        )

    def values_of(s):
        gather_pass(1, s)
        gather_in(1, s)
        each_pair(lambda p: v_pair(s, p))
        for k in range(1, n_tp):
            mom_copy(s, k).start()
        each_pair(lambda p: u_pair(s, p))
        gather_end(1, s)

    def mix_of(s):
        for k in range(1, n_tp):
            mom_copy(s, k).wait_recv()
        shift_columns = square[...].T

        def mix_pair(p):
            moments = mom_own[s, p]
            for k in range(1, n_tp):
                moments = moments + mom_in[s, k - 1, p]
            moments = moments * (1.0 / all_channels)
            columns = jnp.concatenate([moments, jnp.zeros((120, pair), jnp.float32)], axis=0).T
            centre = columns[:, 0:1]
            spread_of = columns[:, 1:2] - centre * centre
            normed_v = (
                (lifted[s, p] - centre) * lax.rsqrt(spread_of + layer_epsilon) * layer_gain[...]
                + layer_shift[...]
            ).astype(jnp.bfloat16)
            for g in range(groups):
                cut = slice(g * group_dim, (g + 1) * group_dim)
                for b in range(pair // SPAN):
                    span = slice(b * SPAN, (b + 1) * SPAN)
                    mixed = jnp.dot(
                        masked[g], normed_v[span, cut], preferred_element_type=jnp.float32
                    )
                    mixed = mixed + shift_columns[:, g : g + 1]
                    gated[s, p, span, cut] = (u_vals[s, p, span, cut] * mixed).astype(jnp.bfloat16)

        each_pair(mix_pair)
        for k in range(1, n_tp):
            mom_copy(s, k).wait_send()

    def guest_values():
        values_of(0)

    def mixer_in():
        row = lax.broadcasted_iota(jnp.int32, (SPAN, SPAN), 0)
        col = lax.broadcasted_iota(jnp.int32, (SPAN, SPAN), 1)
        for g in range(groups):
            masked[g] = jnp.where(row >= col, masked[g].astype(jnp.float32), 0.0).astype(
                jnp.bfloat16
            )
        square[...] = jnp.zeros_like(square)
        square[0:groups, :] = spatial_shift[...]
        arrived(MIX_U)
        arrived(MIX_V)
        when_mid(guest_values)


    between = {
        (GATE, 0): lambda: when_busy(lambda: gather_pass(0, 1)),
        (GATE, 3): lambda: when_mid(lambda: gather_pass(0, 0)),
        (LIFT, 2): lambda: when_busy(gates),
        (DOWN, 0): lambda: when_busy(lifts_own),
        (DOWN, 1): lambda: when_mid(guest_lifts),
        (DOWN, 2): lambda: when_busy(lambda: downs(stops[0], stops[1])),
        (DOWN, 3): lambda: when_busy(lambda: downs(stops[1], stops[2])),
        (MIX_U, 1): lambda: when_busy(far_downs),
        (MIX_U, 3): lambda: when_mid(guest_first),
        (MIX_V, 1): lambda: when_busy(own_first),
        (MIX_DOWN, 1): lambda: when_busy(mixer_in),
    }
    for w in range(6):
        for stage, step in enumerate((early, late)):
            for i in range(w * cuts, (w + 1) * cuts):
                step(i)
                for place, edge in enumerate((w * cuts, (w + 1) * cuts - 1)):
                    if i == edge and (w, 2 * stage + place) in between:
                        between[w, 2 * stage + place]()

    def bands_of(start, stop, run):
        def one(h, carry):
            run(nth_owner(h))
            return carry

        lax.fori_loop(start, stop, one, 0)

    def span_of(s, start, stop):
        bands_of(start, stop, lambda f: products(s, f, gated, MIX_DOWN))
        bands_of(start, stop, lambda f: joins(s, f))

    def second_band(s, f):
        base = resid[s, :, band(f)].astype(jnp.float32)
        resid[s, :, band(f)] = (base + settle(s, f)).astype(jnp.bfloat16)

    def ship(start, stop):
        def one(f):
            second_band(0, f)
            second_copy(f).start()

        bands_of(start, stop, one)

    def mixer_out():
        middle = n_fs // 2

        def guest_in():
            mix_of(0)
            bands_of(1, middle, lambda f: arrived_one(MIX_DOWN, f))
            span_of(0, 0, middle)

        def guest_rest():
            bands_of(middle, n_fs, lambda f: arrived_one(MIX_DOWN, f))
            span_of(0, middle, n_fs)
            ship(0, middle)

        def guest_ship():
            ship(middle, n_fs)
            reduce_end(0)

        when_mid(guest_in)
        values_of(1)
        if spread:
            pl.when(depth > 1)(lambda: arrived(MIX_DOWN))
        else:
            arrived(MIX_DOWN)
        when_mid(guest_rest)
        mix_of(1)
        span_of(1, 0, n_fs)
        when_mid(guest_ship)
        bands_of(0, n_fs, lambda f: second_band(1, f))
        reduce_end(1)

    when_busy(mixer_out)

    def close_guest():
        arrived(GATE)
        arrived(LIFT)
        arrived(DOWN)
        for f in range(n_fs):
            second_copy(f).wait_recv()

    when_end(close_guest)
    def gather_half(k, c):
        ref = rows_last.at[chip, c, core]
        target = other_chip(k) * 2 + core
        return tp_copy(ref, ref, ag_sem.at[0, 1, k - 1, c], ag_sem.at[1, 1, k - 1, c], target)

    def pass_half(k, c):
        ref = rows_last.at[source_chip(k), c, core]
        return tp_copy(ref, ref, agf_sem.at[0, c, k], agf_sem.at[1, c, k], sibling)

    def sib_half(p, f, c):
        rows = pl.ds(c * half, half)
        return tp_copy(
            to_sibling.at[1, p, f, rows], from_sibling.at[1, p, f, rows],
            sib_sem.at[0, c, p, f], sib_sem.at[1, c, p, f], sibling,
        )

    def chip_half(k, f, c):
        rows = pl.ds(c * half, half)
        return tp_copy(
            to_chip.at[1, k - 1, f, rows], from_chip.at[1, k - 1, f, rows],
            chip_sem.at[0, c, k - 1, f], chip_sem.at[1, c, k - 1, f], other_chip(k) * 2 + core,
        )

    normed = norm_rows(resid[1].astype(jnp.float32), gain_after[...])
    for c in range(HALVES):
        rows_last[chip, c, core] = normed[c * half : (c + 1) * half]
        for k in range(1, n_chip):
            gather_half(k, c).start()
        pass_half(0, c).start()

    def last_rows(p, c):
        rows = rows_last[p, c].reshape(2 * half, width)
        gate = jnp.dot(rows, full[GATE][...], preferred_element_type=jnp.float32)
        lift = jnp.dot(rows, full[LIFT][...], preferred_element_type=jnp.float32)
        hidden_last[p, c] = (jax.nn.silu(gate) * lift).astype(jnp.bfloat16)

    def last_products(p, c):
        def one(f, carry):
            part_half[...] = jnp.dot(
                hidden_last[p, c], full[DOWN][f], preferred_element_type=jnp.float32
            ).reshape(part_half.shape)
            rows = pl.ds(c * half, half)
            to_sibling[1, p, f, rows] = part_half[1 - core].astype(jnp.bfloat16)
            hold[1, p, f, rows] = part_half[core]
            sib_half(p, f, c).start()
            return carry

        lax.fori_loop(0, n_fs, one, 0)

    def last_joins(k, c):
        p = other_chip(k)

        def one(f, carry):
            rows = pl.ds(c * half, half)
            sib_half(p, f, c).wait_recv()
            joined = hold[1, p, f, rows] + from_sibling[1, p, f, rows].astype(jnp.float32)
            to_chip[1, k - 1, f, rows] = joined.astype(jnp.bfloat16)
            chip_half(k, f, c).start()
            return carry

        lax.fori_loop(0, n_fs, one, 0)

    for c in range(HALVES):
        pass_half(0, c).wait_recv()
        last_rows(chip, c)

    when_end(lambda: token_copy().wait_send())

    def shipped():
        for f in range(n_fs):
            second_copy(f).wait_send()

    when_mid(shipped)
    sends_done()

    for c in range(HALVES):
        for k in range(1, n_chip):
            gather_half(k, c).wait_recv()
            pass_half(k, c).start()
        for k in range(1, n_chip):
            pass_half(k, c).wait_recv()
            last_rows(other_chip(k), c)
            last_products(other_chip(k), c)
        for k in range(1, n_chip):
            last_joins(k, c)
        last_products(chip, c)
    for f in range(n_fs):
        for c in range(HALVES):
            sib_half(chip, f, c).wait_recv()
        total = hold[1, chip, f] + from_sibling[1, chip, f].astype(jnp.float32)
        for k in range(1, n_chip):
            for c in range(HALVES):
                chip_half(k, f, c).wait_recv()
            total = total + from_chip[1, k - 1, f].astype(jnp.float32)
        base = resid[1, :, band(f)].astype(jnp.float32)
        out[:, band(f)] = (base + 0.5 * total).astype(jnp.bfloat16)
    for c in range(HALVES):
        for k in range(n_chip):
            pass_half(k, c).wait_send()
        for k in range(1, n_chip):
            gather_half(k, c).wait_send()

    def last_sent(f, carry):
        for c in range(HALVES):
            for p in range(n_chip):
                sib_half(p, f, c).wait_send()
            for k in range(1, n_chip):
                chip_half(k, f, c).wait_send()
        return carry

    lax.fori_loop(0, n_fs, last_sent, 0)


def body(
    n_rep,
    n_fs,
    n_tp,
    stream,
    gain_before,
    gain_after,
    proj_gate,
    proj_lift,
    proj_down,
    mixer_gain,
    mixer_u,
    mixer_v,
    layer_gain,
    layer_shift,
    spatial,
    spatial_shift,
    mixer_down,
):
    block, width = stream.shape
    n_chip = n_tp // 2
    pair = 2 * block
    cols = width // n_fs
    units = proj_gate.shape[1]
    channels = mixer_u.shape[1]
    bf16, f32 = jnp.bfloat16, jnp.float32
    shards = (proj_gate, proj_lift, proj_down, mixer_u, mixer_v, mixer_down)
    cuts = cuts_of(shards, n_rep)
    vmem = pl.BlockSpec(memory_space=pltpu.VMEM)
    anywhere = pl.BlockSpec(memory_space=pl.ANY)
    dma = pltpu.SemaphoreType.DMA
    spread_reps = max(n_rep - 1, 1)
    spread_chips = max(n_chip - 1, 1)
    return pl.pallas_call(
        functools.partial(layer_kernel, n_rep, n_fs, n_tp),
        out_shape=pltpu.VMEM((block, width), bf16),
        in_specs=[anywhere] + [vmem] * 5 + [anywhere, vmem] + [anywhere] * 6,
        out_specs=vmem,
        scratch_shapes=[
            pltpu.VMEM(
                (n_fs * w.shape[0], w.shape[1]) if i in BY_ROWS else (n_fs,) + w.shape, bf16
            )
            for i, w in enumerate(shards)
        ]
        + [
            pltpu.VMEM((2, n_chip, pair, width), bf16),
            pltpu.VMEM((2, n_chip, n_fs, block, cols), bf16),
            pltpu.VMEM((2, n_chip, n_fs, block, cols), bf16),
            pltpu.VMEM((2, spread_chips, n_fs, block, cols), bf16),
            pltpu.VMEM((2, spread_chips, n_fs, block, cols), bf16),
            pltpu.VMEM((pair, cols), f32),
            pltpu.VMEM((2, n_chip, n_fs, block, cols), f32),
            pltpu.VMEM((2, n_chip, pair, units), f32),
            pltpu.VMEM((2, n_chip, pair, units), bf16),
            pltpu.VMEM((2, n_chip, pair, channels), f32),
            pltpu.VMEM((2, n_chip, pair, channels), f32),
            pltpu.VMEM((2, n_chip, pair, channels), bf16),
            pltpu.VMEM((n_chip, HALVES, 2, block // HALVES, width), bf16),
            pltpu.VMEM((n_chip, HALVES, 2 * block // HALVES, units), bf16),
            pltpu.VMEM((2, block // HALVES, cols), f32),
            pltpu.VMEM(spatial.shape, bf16),
            pltpu.VMEM((2, n_chip, 8, pair), f32),
            pltpu.VMEM((2, max(n_tp - 1, 1), n_chip, 8, pair), f32),
            pltpu.VMEM((128, SPAN), f32),
            pltpu.VMEM((2, block, width), bf16),
            dma((8,)),
            dma((6, n_fs)),
            dma((6,)),
            dma((6 * cuts, n_fs)),
            dma((6, spread_reps, n_fs)),
            dma((6, spread_reps, n_fs)),
            dma((2, 2, spread_chips, HALVES)),
            dma((2, 2, n_chip)),
            dma((2, 2, n_chip, n_fs)),
            dma((2, 2, spread_chips, n_fs)),
            dma((2, 2, max(n_tp - 1, 1))),
            dma((2,)),
            dma((2, n_fs)),
        ],
        compiler_params=pltpu.CompilerParams(
            collective_id=0, has_side_effects=True, vmem_limit_bytes=60 * 1024 * 1024
        ),
    )(
        stream,
        gain_before.reshape(1, -1),
        gain_after.reshape(1, -1),
        mixer_gain.reshape(1, -1),
        layer_gain.reshape(1, -1),
        layer_shift.reshape(1, -1),
        spatial,
        spatial_shift,
        *shards,
    )


def solution(mesh):
    placed = (
        P(("rep", "fs", "tp"), None),
        P(),
        P(),
        P("fs", "tp"),
        P("fs", "tp"),
        P("tp", "fs"),
        P(),
        P("fs", "tp"),
        P("fs", "tp"),
        P("tp"),
        P("tp"),
        P("tp", None, None),
        P("tp", None),
        P("tp", "fs"),
    )
    sizes = (mesh.shape["rep"], mesh.shape["fs"], mesh.shape["tp"])
    return jax.shard_map(
        functools.partial(body, *sizes),
        mesh=mesh,
        in_specs=placed,
        out_specs=P(("rep", "fs", "tp"), None),
        check_vma=False,
    )
```
